128 devices in a mesh: sp: 16 (over z, x), dp: 8 (over y, core).
Axes of the slice: x: 4, y: 4, z: 4, core: 2. Of those that a mesh axis runs over, the one named last changes fastest.
Arguments:
- tokens: bfloat16 [8, 6144, 2048], P('dp', 'sp'), may hold values from -6 to 6
- q_weight: bfloat16 [2048, 1024], P(('sp', 'dp')), may hold values from -0.13258252 to 0.13258252
- k_weight: bfloat16 [2048, 256], P(('sp', 'dp')), may hold values from -0.13258252 to 0.13258252
- v_weight: bfloat16 [2048, 256], P(('sp', 'dp')), may hold values from -0.125 to 0.125
- out_weight: bfloat16 [1024, 2048], P(None, ('sp', 'dp')), may hold values from -6 to 6
- q_gain: float32 [64], replicated, may hold values from 0.5 to 8
- k_gain: float32 [64], replicated, may hold values from 0.5 to 8
Outputs:
- mixed: bfloat16 [8, 6144, 2048], P('dp', 'sp')
The draws below stay inside these ranges and needn't reach their ends.
All inputs are finite; a program needn't handle non-finite values.
Results may differ from the reference program's by a relative error of at most 0.0055.
The reference program's roundings to bfloat16 on the way (of `values`, `shares` and `attended`) count: a program that leaves them out, or rounds other values in their place, can miss the bound.
Values may be sent and summed in bfloat16 or wider, within the bound.
No kernel may reach another device: no remote copies, remote signals or barrier semaphores. Data moves between devices by JAX's collectives and lax.ppermute only.
A program may use at most 128 MiB of HBM per device.

```python
import math
import jax
import jax.numpy as jnp
from jax import lax

D = 2048
Q_HEADS = 16
KV_HEADS = 4
HEAD_DIM = 64
GRID_W = 64
GROUP = 4
SEQ = 6144
BATCH = 8


def draw_pair(key):
    query_draw = jnp.clip(jax.random.normal(jax.random.fold_in(key, 11), (D, Q_HEADS * HEAD_DIM), jnp.float32), -6.0, 6.0) / math.sqrt(D)
    key_draw = jnp.clip(jax.random.normal(jax.random.fold_in(key, 12), (D, KV_HEADS * HEAD_DIM), jnp.float32), -6.0, 6.0) / math.sqrt(D)
    return (query_draw, key_draw)


def draw_q_weight(key, part):
    return draw_pair(key)[0].astype(jnp.bfloat16)


def draw_k_weight(key, part):
    return draw_pair(key)[1].astype(jnp.bfloat16)


def draw_gain(key):
    return 1.0 + 0.18 * jnp.clip(jax.random.normal(key, (HEAD_DIM,), jnp.float32), -2.5, 2.5)


def draw_q_gain(key, part):
    return draw_gain(jax.random.fold_in(key, 21))


def draw_k_gain(key, part):
    return draw_gain(jax.random.fold_in(key, 22))


def steps_of(rng, dims, shards, smallest, largest):
    def one(axis_at, parts):
        steps = jax.random.uniform(jax.random.fold_in(jax.random.fold_in(rng, 6), axis_at), (parts,), jnp.float32, smallest / len(shards), largest / len(shards))
        return jnp.repeat(jnp.exp(steps), dims[axis_at] // parts).reshape((-1,) + (1,) * (len(dims) - axis_at - 1))

    gain = one(*shards[0])
    for cut in shards[1:]:
        gain = gain * one(*cut)
    return gain


def noise(rng, shape, scale, limit, pieces=(), kind=jnp.bfloat16):
    array = jax.random.normal(rng, shape, jnp.float32) * scale
    if len(pieces) > 0:
        array = steps_of(rng, shape, pieces, -0.22, 0.18) * array
    return jnp.clip(array, min=-limit, max=limit).astype(kind)


def setup_inputs(seed: int = 0) -> dict:
    key_list = jax.random.split(jax.random.key(seed), 8)
    return {
        "tokens": noise(key_list[0], (BATCH, SEQ, D), 1.0, 6.0, ((0, 8), (1, 16))),
        "q_weight": draw_q_weight(jax.random.fold_in(key_list[7], 71), 0),
        "k_weight": draw_k_weight(jax.random.fold_in(key_list[7], 71), 0),
        "v_weight": noise(key_list[3], (D, KV_HEADS * HEAD_DIM), D ** -0.5, 0.125, ((0, 128),)),
        "out_weight": noise(key_list[4], (Q_HEADS * HEAD_DIM, D), (32.0 / (Q_HEADS * HEAD_DIM) ** 0.5), 6.0, ((1, 128),)),
        "q_gain": draw_q_gain(jax.random.fold_in(key_list[7], 71), 0),
        "k_gain": draw_k_gain(jax.random.fold_in(key_list[7], 71), 0),
    }


epsilon = 1e-06
rope_base = 10000.0

def normalize(tensor, gain_vec):
    mean_sq = lax.optimization_barrier(jnp.mean(tensor * tensor, axis=-1, keepdims=True))
    return tensor * lax.rsqrt(mean_sq + epsilon) * gain_vec.astype(jnp.float32)

def rotate(tensor, offset):
    row_count = tensor.shape[0]
    head_width = tensor.shape[2]
    quarter = head_width // 4
    half_width = head_width // 2
    positions = jnp.arange(row_count, dtype=jnp.int32) + offset
    frequency = rope_base ** (-jnp.arange(quarter, dtype=jnp.float32) / quarter)

    def rotate_pair(segment, coords):
        angles = coords.astype(jnp.float32)[:, None] * frequency[None, :]
        cosine = jnp.cos(angles)[:, None, :]
        sine_val = jnp.sin(angles)[:, None, :]
        low_half = segment[..., :quarter]
        high_half = segment[..., quarter:]
        return jnp.concatenate([low_half * cosine - high_half * sine_val, high_half * cosine + low_half * sine_val], axis=-1)
    return jnp.concatenate([rotate_pair(tensor[..., :half_width], positions // GRID_W), rotate_pair(tensor[..., half_width:], positions % GRID_W)], axis=-1)

def attend(query_rows, key_rows, value_rows):
    row_count, head_width = query_rows.shape
    block_rows = math.gcd(row_count, 512)
    score_scale = head_width ** (-0.5)

    def attend_block(segment):
        scores = lax.dot_general(segment, key_rows, (((1,), (1,)), ((), ())), preferred_element_type=jnp.float32) * score_scale
        row_max = lax.optimization_barrier(jnp.max(scores, axis=-1, keepdims=True))
        weights = jnp.exp(scores - row_max)
        shares = (weights / lax.optimization_barrier(jnp.sum(weights, axis=-1, keepdims=True))).astype(jnp.bfloat16)
        return jnp.dot(shares, value_rows, preferred_element_type=jnp.float32).astype(jnp.bfloat16)
    blocks = query_rows.reshape(row_count // block_rows, block_rows, head_width)
    return lax.map(attend_block, blocks).reshape(row_count, head_width)

def reference(tokens, q_weight, k_weight, v_weight, out_weight, q_gain, k_gain):

    def sequence_out(rows_in):
        seq_len = rows_in.shape[0]
        query_raw = jnp.dot(rows_in, q_weight, preferred_element_type=jnp.float32).reshape(seq_len, Q_HEADS, HEAD_DIM)
        key_raw = jnp.dot(rows_in, k_weight, preferred_element_type=jnp.float32).reshape(seq_len, KV_HEADS, HEAD_DIM)
        value_raw = jnp.dot(rows_in, v_weight, preferred_element_type=jnp.float32).reshape(seq_len, KV_HEADS, HEAD_DIM)
        queries = rotate(normalize(query_raw, q_gain), 0).astype(jnp.bfloat16)
        keys = rotate(normalize(key_raw, k_gain), 0).astype(jnp.bfloat16)
        values = value_raw.astype(jnp.bfloat16)
        q_major = jnp.transpose(queries, (1, 0, 2))
        k_major = jnp.transpose(keys, (1, 0, 2))
        v_major = jnp.transpose(values, (1, 0, 2))

        def head_out(head_index):
            kv_index = head_index // GROUP
            q_rows = lax.dynamic_index_in_dim(q_major, head_index, 0, keepdims=False)
            k_rows = lax.dynamic_index_in_dim(k_major, kv_index, 0, keepdims=False)
            v_rows = lax.dynamic_index_in_dim(v_major, kv_index, 0, keepdims=False)
            return attend(q_rows, k_rows, v_rows)
        heads_done = lax.map(head_out, jnp.arange(Q_HEADS, dtype=jnp.int32))
        attended = jnp.transpose(heads_done, (1, 0, 2)).reshape(seq_len, Q_HEADS * HEAD_DIM)
        return jnp.dot(attended, out_weight, preferred_element_type=jnp.float32).astype(jnp.bfloat16)
    return lax.map(sequence_out, tokens)
```

```python
import math

import jax
import jax.numpy as jnp
from jax import lax
from jax.experimental import pallas as pl
from jax.experimental.pallas import tpu as pltpu
from jax.sharding import PartitionSpec as P

GRID_W = 64
LOG2E = 1.4426950408889634
V_ROWS = 80

epsilon = 1e-06
rope_base = 10000.0


def in_one_piece(arrays, axis, dim, along):
    widths = [a.shape[along] for a in arrays]
    both = jnp.concatenate(arrays, axis=along)
    filled = lax.all_gather(both, axis, axis=dim, tiled=True)
    return tuple(jnp.split(filled, [sum(widths[:k]) for k in range(1, len(widths))], axis=along))


def normalize(tensor, gain_vec):
    mean_sq = jnp.mean(tensor * tensor, axis=-1, keepdims=True)
    return tensor * lax.rsqrt(mean_sq + epsilon) * gain_vec


def rotate(tensor, offset):
    row_count = tensor.shape[0]
    head_width = tensor.shape[2]
    quarter = head_width // 4
    half_width = head_width // 2
    positions = jnp.arange(row_count, dtype=jnp.int32) + offset
    frequency = rope_base ** (-jnp.arange(quarter, dtype=jnp.float32) / quarter)

    def rotate_pair(segment, coords):
        angles = coords.astype(jnp.float32)[:, None] * frequency[None, :]
        cosine = jnp.cos(angles)[:, None, :]
        sine_val = jnp.sin(angles)[:, None, :]
        low_half = segment[..., :quarter]
        high_half = segment[..., quarter:]
        return jnp.concatenate(
            [low_half * cosine - high_half * sine_val, high_half * cosine + low_half * sine_val],
            axis=-1,
        )

    return jnp.concatenate(
        [
            rotate_pair(tensor[..., :half_width], positions // GRID_W),
            rotate_pair(tensor[..., half_width:], positions % GRID_W),
        ],
        axis=-1,
    )


def _attend_call(kern, q_t, k2, v_t, q_block, name):
    rows = q_t.shape[1]
    keys = k2.shape[0]
    return pl.pallas_call(
        kern,
        grid=(rows // q_block,),
        in_specs=[
            pl.BlockSpec((64, q_block), lambda i: (0, i)),
            pl.BlockSpec((keys, 128), lambda i: (0, 0)),
            pl.BlockSpec((V_ROWS, keys), lambda i: (0, 0)),
        ],
        out_specs=pl.BlockSpec((64, q_block), lambda i: (0, i)),
        out_shape=jax.ShapeDtypeStruct((64, rows), jnp.bfloat16),
        compiler_params=pltpu.CompilerParams(vmem_limit_bytes=56 * 2**20),
        name=name,
    )(q_t, k2, v_t)


def attend_bounded(q_t, k2, v_t):
    key_tile = 1024

    def kern(q_ref, k_ref, v_ref, o_ref):
        scaled = q_ref[...].astype(jnp.float32) * (0.125 * LOG2E)
        high = scaled.astype(jnp.bfloat16)
        low = (scaled - high.astype(jnp.float32)).astype(jnp.bfloat16)
        q2 = jnp.concatenate([high, low], axis=0)
        acc = jnp.zeros((V_ROWS, q2.shape[1]), jnp.float32)
        for u in range(k_ref.shape[0] // key_tile):
            rows = pl.ds(u * key_tile, key_tile)
            scores = jnp.dot(k_ref[rows, :], q2, preferred_element_type=jnp.float32)
            weights = jnp.exp2(scores).astype(jnp.bfloat16)
            acc = acc + jnp.dot(v_ref[:, rows], weights, preferred_element_type=jnp.float32)
        o_ref[...] = (acc[:64] / acc[64:65]).astype(jnp.bfloat16)

    return _attend_call(kern, q_t, k2, v_t, 1024, "attend_bounded")


def attend_running_max(q_t, k2, v_t):
    key_tile = 512

    def kern(q_ref, k_ref, v_ref, o_ref):
        q = q_ref[...]

        def step(u, carry):
            top, acc = carry
            rows = pl.ds(pl.multiple_of(u * key_tile, key_tile), key_tile)
            scores = jnp.dot(k_ref[rows, :64], q, preferred_element_type=jnp.float32) * 0.125
            new_top = jnp.maximum(top, jnp.max(scores, axis=0, keepdims=True))
            weights = jnp.exp(scores - new_top).astype(jnp.bfloat16)
            part = jnp.dot(v_ref[:, rows], weights, preferred_element_type=jnp.float32)
            return new_top, acc * jnp.exp(top - new_top) + part

        start = (
            jnp.full((1, q.shape[1]), -1e30, jnp.float32),
            jnp.zeros((V_ROWS, q.shape[1]), jnp.float32),
        )
        _, acc = lax.fori_loop(0, k_ref.shape[0] // key_tile, step, start)
        o_ref[...] = (acc[:64] / acc[64:65]).astype(jnp.bfloat16)

    return _attend_call(kern, q_t, k2, v_t, 512, "attend_running_max")


def attend(query_rows, key_rows, value_rows, bounded):
    keys = key_rows.shape[0]
    q_t = query_rows.T
    k2 = jnp.concatenate([key_rows, key_rows], axis=1)
    v_t = jnp.concatenate(
        [
            value_rows.T,
            jnp.ones((1, keys), jnp.bfloat16),
            jnp.zeros((V_ROWS - 65, keys), jnp.bfloat16),
        ],
        axis=0,
    )
    return lax.cond(bounded, attend_bounded, attend_running_max, q_t, k2, v_t).T


def per_device(tokens, q_weight, k_weight, v_weight, out_weight, q_gain, k_gain):
    rows_in = tokens[0]
    tok_count = rows_in.shape[0]
    head_width = q_gain.shape[0]
    q_width = out_weight.shape[0]
    kv_width = k_weight.shape[1]
    q_heads = q_width // head_width
    kv_heads = kv_width // head_width
    group_size = q_heads // kv_heads
    offset = lax.axis_index("sp") * tok_count
    bounded = 8.0 * jnp.max(jnp.abs(q_gain)) * jnp.max(jnp.abs(k_gain)) <= 60.0
    weight_rows = in_one_piece((q_weight, k_weight, v_weight), ("sp", "dp"), 0, 1)
    query_raw, key_raw, value_raw = tuple(
        (
            jnp.dot(rows_in, rows_part, preferred_element_type=jnp.float32)
            for rows_part in weight_rows
        )
    )
    queries = rotate(
        normalize(query_raw.reshape(tok_count, q_heads, head_width), q_gain), offset
    ).astype(jnp.bfloat16)
    keys_rot = rotate(
        normalize(key_raw.reshape(tok_count, kv_heads, head_width), k_gain), offset
    ).astype(jnp.bfloat16)
    values_dev = value_raw.astype(jnp.bfloat16)
    keys_wide = jnp.broadcast_to(
        keys_rot[:, :, None, :], (tok_count, kv_heads, group_size, head_width)
    ).reshape(tok_count, q_width)
    values_wide = jnp.broadcast_to(
        values_dev.reshape(tok_count, kv_heads, 1, head_width),
        (tok_count, kv_heads, group_size, head_width),
    ).reshape(tok_count, q_width)
    q_local, k_local, v_local = (
        lax.all_to_all(
            queries.reshape(tok_count, q_width), "sp", split_axis=1, concat_axis=0, tiled=True
        ),
        lax.all_to_all(keys_wide, "sp", split_axis=1, concat_axis=0, tiled=True),
        lax.all_to_all(values_wide, "sp", split_axis=1, concat_axis=0, tiled=True),
    )
    outputs = attend(q_local, k_local, v_local, bounded)
    attended = lax.all_to_all(outputs, "sp", split_axis=0, concat_axis=1, tiled=True)
    result = jnp.dot(
        attended,
        lax.all_gather(out_weight, ("sp", "dp"), axis=1, tiled=True),
        preferred_element_type=jnp.float32,
    ).astype(jnp.bfloat16)
    return result[None]


def solution(mesh):
    return jax.shard_map(
        per_device,
        mesh=mesh,
        in_specs=(
            P("dp", "sp", None),
            P(("sp", "dp"), None),
            P(("sp", "dp"), None),
            P(("sp", "dp"), None),
            P(None, ("sp", "dp")),
            P(),
            P(),
        ),
        out_specs=P("dp", "sp", None),
        check_vma=False,
    )
```

```python
import jax
import jax.numpy as jnp
import numpy as np
from jax import lax
from jax.experimental import pallas as pl
from jax.experimental.pallas import tpu as pltpu
from jax.sharding import PartitionSpec as P

GRID_W = 64
LOG2E = 1.4426950408889634
V_ROWS = 80
HEAD = 64
KV_HEADS = 4
GROUP = 4
TOK = 384
WIDE = 384
QKV = KV_HEADS * WIDE
OUT_IN = 1024
MODEL = 2048

epsilon = 1e-06
rope_base = 10000.0

AXES = ("sp", "dp")
DEVICE = np.arange(128).reshape(4, 4, 4, 2)
SHIFTS = (0, -1, 1, 2)


def lines(axis, core):
    return np.moveaxis(DEVICE[..., core], "zxy".index(axis), -1).reshape(-1, 4).tolist()


def shift_pairs(axis_of_core, step):
    pairs = []
    for core, axis in enumerate(axis_of_core):
        for line in lines(axis, core):
            pairs += [(line[i], line[(i + step) % 4]) for i in range(4)]
    return pairs


INNER = ("x", "z")
OUTER = ("z", "x")
SWAP = [(int(i), int(i) ^ 1) for i in range(128)]
EXCHANGE = lines("x", 0) + lines("z", 1)


def shift(array, axis_of_core, step):
    return lax.ppermute(array, AXES, shift_pairs(axis_of_core, step))


def swap(array):
    return lax.ppermute(array, AXES, SWAP)


def ring(array, axis_of_core):
    half = array.shape[0] // 2
    left = shift(array, axis_of_core, 1)
    right = shift(array, axis_of_core, -1)
    far_top = shift(left[:half], axis_of_core, 1)
    far_bottom = shift(right[half:], axis_of_core, -1)
    return left, right, far_top, far_bottom


def row_of(where, core, outer, inner, y_step):
    z, x, y = where[0], where[1], where[2]
    a = SHIFTS[outer]
    b = SHIFTS[inner]
    first = core == 0
    z_at = (z + jnp.where(first, a, b) + 4) % 4
    x_at = (x + jnp.where(first, b, a) + 4) % 4
    y_at = (y + SHIFTS[y_step] + 4) % 4
    return (z_at * 4 + x_at) * 128 + y_at * 32 + core * 16


def lay_out(where, mine, theirs, full_ref):
    for pieces, core in ((mine, where[3]), (theirs, 1 - where[3])):
        for outer in range(4):
            for inner in range(4):
                for y_step in range(4):
                    row = inner * 64 + y_step * 16
                    if outer < 3:
                        source = pieces[outer]
                    else:
                        source = pieces[3 + row // 128]
                        row = row % 128
                    at = pl.multiple_of(row_of(where, core, outer, inner, y_step), 16)
                    full_ref[pl.ds(at, 16), :] = source[row : row + 16, :]


def project(where, tokens, mine, theirs, tables, q_gain, k_gain):
    def kern(where_ref, tok_ref, *refs):
        own = refs[:5]
        other = refs[5:10]
        table_ref, qg_ref, kg_ref, out_ref, full_ref = refs[10:]
        place = [where_ref[i] for i in range(4)]
        lay_out(place, own, other, full_ref)
        raw = jnp.dot(tok_ref[...], full_ref[...], preferred_element_type=jnp.float32)
        flat = raw.T
        cos_r, sin_r = table_ref[0:16, :], table_ref[16:32, :]
        cos_c, sin_c = table_ref[32:48, :], table_ref[48:64, :]
        for head in range(GROUP + 1):
            v = flat[head * HEAD : (head + 1) * HEAD, :]
            gain = qg_ref[...] if head < GROUP else kg_ref[...]
            mean_sq = jnp.mean(v * v, axis=0, keepdims=True)
            v = v * lax.rsqrt(mean_sq + epsilon) * gain
            a, b, c, d = v[0:16], v[16:32], v[32:48], v[48:64]
            turned = jnp.concatenate(
                [
                    a * cos_r - b * sin_r,
                    b * cos_r + a * sin_r,
                    c * cos_c - d * sin_c,
                    d * cos_c + c * sin_c,
                ],
                axis=0,
            )
            out_ref[0, head * HEAD : (head + 1) * HEAD, :] = turned.astype(jnp.bfloat16)
        out_ref[0, (GROUP + 1) * HEAD :, :] = flat[(GROUP + 1) * HEAD :, :].astype(jnp.bfloat16)

    def piece(array):
        return pl.BlockSpec((array.shape[0], WIDE), lambda g: (0, g))

    return pl.pallas_call(
        kern,
        grid=(KV_HEADS,),
        in_specs=[
            pl.BlockSpec(memory_space=pltpu.SMEM),
            pl.BlockSpec((TOK, MODEL), lambda g: (0, 0)),
            *[piece(a) for a in mine],
            *[piece(a) for a in theirs],
            pl.BlockSpec((HEAD, TOK), lambda g: (0, 0)),
            pl.BlockSpec((HEAD, 1), lambda g: (0, 0)),
            pl.BlockSpec((HEAD, 1), lambda g: (0, 0)),
        ],
        out_specs=pl.BlockSpec((1, WIDE, TOK), lambda g: (g, 0, 0)),
        out_shape=jax.ShapeDtypeStruct((KV_HEADS, WIDE, TOK), jnp.bfloat16),
        scratch_shapes=[pltpu.VMEM((MODEL, WIDE), jnp.bfloat16)],
        compiler_params=pltpu.CompilerParams(vmem_limit_bytes=48 * 2**20),
        name="project",
    )(where, tokens, *mine, *theirs, tables, q_gain, k_gain)


def attend(bounded, qkv, others):
    keys = 16 * TOK
    tile = 1024

    def kern(flag_ref, q_ref, own_ref, left_ref, right_ref, top_ref, bottom_ref, o_ref, k_ref, v_ref):
        @pl.when(pl.program_id(0) == 0)
        def _():
            at = 0
            for source in (own_ref, left_ref, right_ref, top_ref, bottom_ref):
                for i in range(source.shape[0]):
                    k = source[i, 0:HEAD, :]
                    k_ref[at : at + TOK, :] = jnp.concatenate([k, k], axis=0).T
                    v_ref[0:HEAD, at : at + TOK] = source[i, HEAD : 2 * HEAD, :]
                    at += TOK
            row = lax.broadcasted_iota(jnp.int32, (V_ROWS - HEAD, keys), 0)
            v_ref[HEAD:, :] = jnp.where(row == 0, 1.0, 0.0).astype(jnp.bfloat16)

        q = jnp.concatenate([q_ref[i] for i in range(4)], axis=1)

        def finish(acc):
            done = (acc[:HEAD] / acc[HEAD : HEAD + 1]).astype(jnp.bfloat16)
            for i in range(4):
                o_ref[i] = done[:, i * TOK : (i + 1) * TOK]

        @pl.when(flag_ref[0] == 1)
        def _():
            scaled = q.astype(jnp.float32) * (0.125 * LOG2E)
            high = scaled.astype(jnp.bfloat16)
            low = (scaled - high.astype(jnp.float32)).astype(jnp.bfloat16)
            q2 = jnp.concatenate([high, low], axis=0)
            acc = jnp.zeros((V_ROWS, 4 * TOK), jnp.float32)
            for u in range(keys // tile):
                rows = pl.ds(u * tile, tile)
                scores = jnp.dot(k_ref[rows, :], q2, preferred_element_type=jnp.float32)
                weights = jnp.exp2(scores).astype(jnp.bfloat16)
                acc = acc + jnp.dot(v_ref[:, rows], weights, preferred_element_type=jnp.float32)
            finish(acc)

        @pl.when(flag_ref[0] != 1)
        def _():
            step_rows = 512

            def step(u, carry):
                top, acc = carry
                rows = pl.ds(pl.multiple_of(u * step_rows, step_rows), step_rows)
                scores = (
                    jnp.dot(k_ref[rows, :HEAD], q, preferred_element_type=jnp.float32) * 0.125
                )
                new_top = jnp.maximum(top, jnp.max(scores, axis=0, keepdims=True))
                weights = jnp.exp(scores - new_top).astype(jnp.bfloat16)
                part = jnp.dot(v_ref[:, rows], weights, preferred_element_type=jnp.float32)
                return new_top, acc * jnp.exp(top - new_top) + part

            start = (
                jnp.full((1, 4 * TOK), -1e30, jnp.float32),
                jnp.zeros((V_ROWS, 4 * TOK), jnp.float32),
            )
            finish(lax.fori_loop(0, keys // step_rows, step, start)[1])

    def whole(array):
        return pl.BlockSpec(array.shape, lambda h: (0, 0, 0))

    return pl.pallas_call(
        kern,
        grid=(GROUP,),
        in_specs=[
            pl.BlockSpec(memory_space=pltpu.SMEM),
            pl.BlockSpec((4, HEAD, TOK), lambda h: (0, h, 0)),
            pl.BlockSpec((4, 2 * HEAD, TOK), lambda h: (0, 2, 0)),
            *[whole(a) for a in others],
        ],
        out_specs=pl.BlockSpec((4, HEAD, TOK), lambda h: (0, h, 0)),
        out_shape=jax.ShapeDtypeStruct((4, GROUP * HEAD, TOK), jnp.bfloat16),
        scratch_shapes=[
            pltpu.VMEM((keys, 2 * HEAD), jnp.bfloat16),
            pltpu.VMEM((V_ROWS, keys), jnp.bfloat16),
        ],
        compiler_params=pltpu.CompilerParams(vmem_limit_bytes=56 * 2**20),
        name="attend",
    )(bounded, qkv, qkv, *others)


def mix(where, attended, mine, theirs):
    def kern(where_ref, att_ref, *refs):
        out_ref, full_ref = refs[10:]
        place = [where_ref[i] for i in range(4)]
        lay_out(place, refs[:5], refs[5:10], full_ref)
        rows = att_ref[...].T
        out_ref[...] = lax.dot_general(
            rows, full_ref[...], (((1,), (1,)), ((), ())), preferred_element_type=jnp.float32
        ).astype(jnp.bfloat16)

    def piece(array):
        return pl.BlockSpec(array.shape, lambda: (0, 0))

    return pl.pallas_call(
        kern,
        in_specs=[
            pl.BlockSpec(memory_space=pltpu.SMEM),
            pl.BlockSpec((OUT_IN, TOK), lambda: (0, 0)),
            *[piece(a) for a in mine],
            *[piece(a) for a in theirs],
        ],
        out_specs=pl.BlockSpec((TOK, MODEL), lambda: (0, 0)),
        out_shape=jax.ShapeDtypeStruct((TOK, MODEL), jnp.bfloat16),
        scratch_shapes=[pltpu.VMEM((MODEL, OUT_IN), jnp.bfloat16)],
        compiler_params=pltpu.CompilerParams(vmem_limit_bytes=48 * 2**20),
        name="mix",
    )(where, attended, *mine, *theirs)


def rotation_tables(offset):
    quarter = HEAD // 4
    positions = jnp.arange(TOK, dtype=jnp.int32) + offset
    frequency = rope_base ** (-jnp.arange(quarter, dtype=jnp.float32) / quarter)
    parts = []
    for coords in (positions // GRID_W, positions % GRID_W):
        angles = coords.astype(jnp.float32)[None, :] * frequency[:, None]
        parts += [jnp.cos(angles), jnp.sin(angles)]
    return jnp.concatenate(parts, axis=0)


def per_device(tokens, q_weight, k_weight, v_weight, out_weight, q_gain, k_gain):
    sp = lax.axis_index("sp")
    dp = lax.axis_index("dp")
    where = jnp.stack([sp // 4, sp % 4, dp // 2, dp % 2]).astype(jnp.int32)
    bounded = 8.0 * jnp.max(jnp.abs(q_gain)) * jnp.max(jnp.abs(k_gain)) <= 60.0
    tables = rotation_tables(sp * TOK)

    columns = []
    for g in range(KV_HEADS):
        columns += [
            q_weight[:, 256 * g : 256 * (g + 1)],
            k_weight[:, HEAD * g : HEAD * (g + 1)],
            v_weight[:, HEAD * g : HEAD * (g + 1)],
        ]
    block = jnp.concatenate([*columns, out_weight.T], axis=1)
    block = jnp.concatenate([block, *[shift(block, ("y", "y"), -s) for s in SHIFTS[1:]]], axis=0)
    block = jnp.concatenate([block, *ring(block, INNER)], axis=0)

    in_own = block[:, :QKV]
    in_mine = (in_own, *ring(in_own, OUTER))
    in_theirs = tuple(swap(a) for a in in_mine)
    qkv = project(
        where, tokens[0], in_mine, in_theirs, tables, q_gain.reshape(HEAD, 1), k_gain.reshape(HEAD, 1)
    )

    qkv = lax.all_to_all(
        qkv, AXES, split_axis=0, concat_axis=0, tiled=True, axis_index_groups=EXCHANGE
    )
    others = ring(qkv[:, GROUP * HEAD :, :], OUTER)
    out_own = block[:, QKV:]
    out_mine = (out_own, *ring(out_own, OUTER))
    out_theirs = tuple(swap(a) for a in out_mine)
    attended = attend(bounded.astype(jnp.int32).reshape(1), qkv, others)
    attended = lax.all_to_all(
        attended, AXES, split_axis=0, concat_axis=0, tiled=True, axis_index_groups=EXCHANGE
    )
    return mix(where, attended.reshape(OUT_IN, TOK), out_mine, out_theirs)[None]


def solution(mesh):
    return jax.shard_map(
        per_device,
        mesh=mesh,
        in_specs=(
            P("dp", "sp", None),
            P(("sp", "dp"), None),
            P(("sp", "dp"), None),
            P(("sp", "dp"), None),
            P(None, ("sp", "dp")),
            P(),
            P(),
        ),
        out_specs=P("dp", "sp", None),
        check_vma=False,
    )
```

```python
import jax
import jax.numpy as jnp
import numpy as np
from jax import lax
from jax.experimental import pallas as pl
from jax.experimental.pallas import tpu as pltpu
from jax.sharding import PartitionSpec as P

GRID_W = 64
LOG2E = 1.4426950408889634
V_ROWS = 80
ATTEND_VMEM = 24 * 2**20
HEAD = 64
KV_HEADS = 4
GROUP = 4
TOK = 384
WIDE = 384
QKV = KV_HEADS * WIDE
OUT_IN = 1024
MODEL = 2048

epsilon = 1e-06
rope_base = 10000.0

AXES = ("sp", "dp")
DEVICE = np.arange(128).reshape(4, 4, 4, 2)
SHIFTS = (0, -1, 1, 2)


def lines(axis, core):
    return np.moveaxis(DEVICE[..., core], "zxy".index(axis), -1).reshape(-1, 4).tolist()


def shift_pairs(axis_of_core, step):
    pairs = []
    for core, axis in enumerate(axis_of_core):
        for line in lines(axis, core):
            pairs += [(line[i], line[(i + step) % 4]) for i in range(4)]
    return pairs


INNER = ("x", "z")
OUTER = ("z", "x")
SWAP = [(int(i), int(i) ^ 1) for i in range(128)]
EXCHANGE = lines("x", 0) + lines("z", 1)


def shift(array, axis_of_core, step):
    return lax.ppermute(array, AXES, shift_pairs(axis_of_core, step))


def pair(array, axis_of_core, far):
    pairs = []
    for core, axis in enumerate(axis_of_core):
        for line in lines(axis, core):
            pairs += [(line[i], line[3 - i if far else i ^ 1]) for i in range(4)]
    return lax.ppermute(array, AXES, pairs)


def swap(array):
    return lax.ppermute(array, AXES, SWAP)


def ring(top, bottom, axis_of_core):
    left_top = shift(top, axis_of_core, 1)
    right_bottom = shift(bottom, axis_of_core, -1)
    left_bottom = shift(bottom, axis_of_core, 1)
    right_top = shift(top, axis_of_core, -1)
    far_top = shift(left_top, axis_of_core, 1)
    far_bottom = shift(right_bottom, axis_of_core, -1)
    return left_top, left_bottom, right_top, right_bottom, far_top, far_bottom


def ring_order(at):
    return [(at + s + 4) % 4 for s in SHIFTS]


def pair_order(at):
    near = at + 1 - 2 * (at % 2)
    return [at, near, 3 - at, 3 - near]


def lay_out(where, mine, theirs, full_ref, outer_order):
    z, x, y, own_core = where
    y_at = ring_order(y)
    for pieces, core in ((mine, own_core), (theirs, 1 - own_core)):
        first = core == 0
        outer_at = outer_order(jnp.where(first, z, x))
        inner_at = pair_order(jnp.where(first, x, z))
        stack = [(p, r) for p in pieces for r in range(0, p.shape[0], 16)]
        for outer in range(4):
            for inner in range(4):
                z_at = jnp.where(first, outer_at[outer], inner_at[inner])
                x_at = jnp.where(first, inner_at[inner], outer_at[outer])
                base = (z_at * 4 + x_at) * 128 + core * 16
                for step in range(4):
                    source, row = stack[outer * 16 + inner * 4 + step]
                    at = pl.multiple_of(base + y_at[step] * 32, 16)
                    full_ref[pl.ds(at, 16), :] = source[row : row + 16, :]


def column(row):
    size = row.shape[1]
    diagonal = lax.broadcasted_iota(jnp.int32, (size, size), 0) == lax.broadcasted_iota(
        jnp.int32, (size, size), 1
    )
    return jnp.sum(jnp.where(diagonal, row, 0.0), axis=1, keepdims=True)


def project(where, tokens, mine, theirs, tables, q_gain, k_gain):
    count = len(mine)

    def kern(where_ref, tok_ref, *refs):
        table_ref, qg_ref, kg_ref, out_ref, full_ref = refs[2 * count :]
        place = [where_ref[i] for i in range(4)]
        lay_out(place, refs[:count], refs[count : 2 * count], full_ref, ring_order)
        cos_r, sin_r = table_ref[0:16, :], table_ref[16:32, :]
        cos_c, sin_c = table_ref[32:48, :], table_ref[48:64, :]
        gains = (column(qg_ref[...]), column(kg_ref[...]))
        tok = tok_ref[...]
        heads = GROUP * KV_HEADS
        for pair in range((heads + 2 * KV_HEADS) // 2):
            cols = slice(pair * 2 * HEAD, (pair + 1) * 2 * HEAD)
            if pair % 2 == 0:
                both = slice(cols.start, cols.start + 4 * HEAD)
                raw = jnp.dot(tok, full_ref[:, both], preferred_element_type=jnp.float32)
            flat = raw[:, (pair % 2) * 2 * HEAD : (pair % 2 + 1) * 2 * HEAD].T
            for i in range(2):
                head = 2 * pair + i
                v = flat[i * HEAD : (i + 1) * HEAD, :]
                if head < heads + KV_HEADS:
                    mean_sq = jnp.mean(v * v, axis=0, keepdims=True)
                    v = v * lax.rsqrt(mean_sq + epsilon) * gains[head // heads]
                    a, b, c, d = v[0:16], v[16:32], v[32:48], v[48:64]
                    v = jnp.concatenate(
                        [
                            a * cos_r - b * sin_r,
                            b * cos_r + a * sin_r,
                            c * cos_c - d * sin_c,
                            d * cos_c + c * sin_c,
                        ],
                        axis=0,
                    )
                if head < heads:
                    group, at = head // GROUP, head % GROUP
                else:
                    group, at = head % KV_HEADS, GROUP + (head - heads) // KV_HEADS
                out_ref[group, at * HEAD : (at + 1) * HEAD, :] = v.astype(jnp.bfloat16)

    return pl.pallas_call(
        kern,
        in_specs=[pl.BlockSpec(memory_space=pltpu.SMEM)]
        + [pl.BlockSpec(memory_space=pltpu.VMEM)] * (2 * count + 4),
        out_specs=pl.BlockSpec(memory_space=pltpu.VMEM),
        out_shape=jax.ShapeDtypeStruct((KV_HEADS, WIDE, TOK), jnp.bfloat16),
        scratch_shapes=[pltpu.VMEM((MODEL, QKV), jnp.bfloat16)],
        compiler_params=pltpu.CompilerParams(vmem_limit_bytes=28 * 2**20),
        cost_estimate=pl.CostEstimate(
            flops=2 * TOK * MODEL * QKV, bytes_accessed=2 * MODEL * QKV, transcendentals=0
        ),
        name="project",
    )(where, tokens, *mine, *theirs, tables, q_gain, k_gain)


def attend(q_gain, k_gain, qkv, pieces, before):
    keys = sum(p.shape[0] for p in pieces) * TOK
    tile = 1024
    wide = 4 * TOK
    last = before is not None

    def kern(qg_ref, kg_ref, q_ref, *refs):
        sources = refs[: len(pieces)]
        rest = refs[len(pieces) :]
        if last:
            acc_in, top_in, o_ref, k_ref, v_ref = rest
        else:
            acc_out, top_out, k_ref, v_ref = rest

        @pl.when(pl.program_id(0) == 0)
        def _():
            at = 0
            for source in sources:
                for i in range(source.shape[0]):
                    k = source[i, 0:HEAD, :]
                    k_ref[at : at + TOK, :] = jnp.concatenate([k, k], axis=0).T
                    v_ref[0:HEAD, at : at + TOK] = source[i, HEAD : 2 * HEAD, :]
                    at += TOK
            row = lax.broadcasted_iota(jnp.int32, (V_ROWS - HEAD, keys), 0)
            v_ref[HEAD:, :] = jnp.where(row == 0, 1.0, 0.0).astype(jnp.bfloat16)

        q = jnp.concatenate([q_ref[i] for i in range(4)], axis=1)
        limit = 8.0 * jnp.max(jnp.abs(qg_ref[...])) * jnp.max(jnp.abs(kg_ref[...]))

        def finish(acc, top):
            if last:
                done = (acc[:HEAD] / acc[HEAD : HEAD + 1]).astype(jnp.bfloat16)
                for i in range(4):
                    o_ref[i] = done[:, i * TOK : (i + 1) * TOK]
            else:
                acc_out[0] = acc
                top_out[0] = top

        @pl.when(limit <= 60.0)
        def _():
            scaled = q.astype(jnp.float32) * (0.125 * LOG2E)
            high = scaled.astype(jnp.bfloat16)
            low = (scaled - high.astype(jnp.float32)).astype(jnp.bfloat16)
            q2 = jnp.concatenate([high, low], axis=0)
            acc = acc_in[0] if last else jnp.zeros((V_ROWS, wide), jnp.float32)
            for u in range(keys // tile):
                rows = pl.ds(u * tile, tile)
                scores = jnp.dot(k_ref[rows, :], q2, preferred_element_type=jnp.float32)
                weights = jnp.exp2(scores).astype(jnp.bfloat16)
                acc = acc + jnp.dot(v_ref[:, rows], weights, preferred_element_type=jnp.float32)
            finish(acc, jnp.zeros((8, wide), jnp.float32))

        @pl.when(jnp.logical_not(limit <= 60.0))
        def _():
            step_rows = 512

            def step(u, carry):
                top, acc = carry
                rows = pl.ds(pl.multiple_of(u * step_rows, step_rows), step_rows)
                scores = (
                    jnp.dot(k_ref[rows, :HEAD], q, preferred_element_type=jnp.float32) * 0.125
                )
                new_top = jnp.maximum(top, jnp.max(scores, axis=0, keepdims=True))
                weights = jnp.exp(scores - new_top).astype(jnp.bfloat16)
                part = jnp.dot(v_ref[:, rows], weights, preferred_element_type=jnp.float32)
                return new_top, acc * jnp.exp(top - new_top) + part

            if last:
                start = (top_in[0, 0:1, :], acc_in[0])
            else:
                start = (
                    jnp.full((1, wide), -1e30, jnp.float32),
                    jnp.zeros((V_ROWS, wide), jnp.float32),
                )
            top, acc = lax.fori_loop(0, keys // step_rows, step, start)
            finish(acc, jnp.broadcast_to(top, (8, wide)))

    def whole(array, at):
        return pl.BlockSpec((array.shape[0], 2 * HEAD, TOK), lambda h: (0, at, 0))

    sums = [
        pl.BlockSpec((1, V_ROWS, wide), lambda h: (h, 0, 0)),
        pl.BlockSpec((1, 8, wide), lambda h: (h, 0, 0)),
    ]
    gain = pl.BlockSpec((1, HEAD), lambda h: (0, 0))
    return pl.pallas_call(
        kern,
        grid=(GROUP,),
        in_specs=[
            gain,
            gain,
            pl.BlockSpec((4, HEAD, TOK), lambda h: (0, h, 0)),
            *[whole(p, 0 if p.shape[1] == 2 * HEAD else 2) for p in pieces],
            *(sums if last else []),
        ],
        out_specs=pl.BlockSpec((4, HEAD, TOK), lambda h: (0, h, 0)) if last else sums,
        out_shape=jax.ShapeDtypeStruct((4, GROUP * HEAD, TOK), jnp.bfloat16)
        if last
        else [
            jax.ShapeDtypeStruct((GROUP, V_ROWS, wide), jnp.float32),
            jax.ShapeDtypeStruct((GROUP, 8, wide), jnp.float32),
        ],
        scratch_shapes=[
            pltpu.VMEM((keys, 2 * HEAD), jnp.bfloat16),
            pltpu.VMEM((V_ROWS, keys), jnp.bfloat16),
        ],
        compiler_params=pltpu.CompilerParams(vmem_limit_bytes=ATTEND_VMEM),
        cost_estimate=pl.CostEstimate(
            flops=16 * keys * wide * 256 * 2,
            bytes_accessed=2 * keys * 2 * HEAD,
            transcendentals=GROUP * keys * wide,
        ),
        name="attend_last" if last else "attend_first",
    )(q_gain, k_gain, qkv, *pieces, *(before or []))


def mix(where, attended, mine, theirs):
    count = len(mine)

    def kern(where_ref, att_ref, *refs):
        out_ref, full_ref = refs[2 * count :]
        place = [where_ref[i] for i in range(4)]
        lay_out(place, refs[:count], refs[count : 2 * count], full_ref, pair_order)
        rows = att_ref[...].T
        out_ref[...] = lax.dot_general(
            rows, full_ref[...], (((1,), (1,)), ((), ())), preferred_element_type=jnp.float32
        ).astype(jnp.bfloat16)

    def piece(array):
        return pl.BlockSpec(array.shape, lambda: (0, 0))

    return pl.pallas_call(
        kern,
        in_specs=[
            pl.BlockSpec(memory_space=pltpu.SMEM),
            pl.BlockSpec((OUT_IN, TOK), lambda: (0, 0)),
            *[piece(a) for a in mine],
            *[piece(a) for a in theirs],
        ],
        out_specs=pl.BlockSpec((TOK, MODEL), lambda: (0, 0)),
        out_shape=jax.ShapeDtypeStruct((TOK, MODEL), jnp.bfloat16),
        scratch_shapes=[pltpu.VMEM((MODEL, OUT_IN), jnp.bfloat16)],
        compiler_params=pltpu.CompilerParams(vmem_limit_bytes=24 * 2**20),
        cost_estimate=pl.CostEstimate(
            flops=2 * TOK * MODEL * OUT_IN, bytes_accessed=2 * MODEL * OUT_IN, transcendentals=0
        ),
        name="mix",
    )(where, attended, *mine, *theirs)


def rotation_tables(offset):
    quarter = HEAD // 4
    positions = jnp.arange(TOK, dtype=jnp.int32) + offset
    frequency = rope_base ** (-jnp.arange(quarter, dtype=jnp.float32) / quarter)
    parts = []
    for coords in (positions // GRID_W, positions % GRID_W):
        angles = coords.astype(jnp.float32)[None, :] * frequency[:, None]
        parts += [jnp.cos(angles), jnp.sin(angles)]
    return jnp.concatenate(parts, axis=0)


def per_device(tokens, q_weight, k_weight, v_weight, out_weight, q_gain, k_gain):
    sp = lax.axis_index("sp")
    dp = lax.axis_index("dp")
    where = jnp.stack([sp // 4, sp % 4, dp // 2, dp % 2]).astype(jnp.int32)
    tables = rotation_tables(sp * TOK)
    q_row = q_gain.reshape(1, HEAD)
    k_row = k_gain.reshape(1, HEAD)

    own = jnp.concatenate([q_weight, k_weight, v_weight, out_weight.T], axis=1)
    block = jnp.concatenate([own, *[shift(own, ("y", "y"), -s) for s in SHIFTS[1:]]], axis=0)
    near = pair(block, INNER, False)
    half = jnp.concatenate([block, near], axis=0)
    other = pair(half, INNER, True)
    tables, where, half, other = lax.optimization_barrier((tables, where, half, other))

    in_mine = [half[:, :QKV], other[:, :QKV]]
    in_mine += ring(*in_mine, OUTER)
    in_theirs = [swap(a) for a in in_mine]
    qkv = project(where, tokens[0], in_mine, in_theirs, tables, q_row, k_row)

    out_own = jnp.concatenate([half[:, QKV:], other[:, QKV:]], axis=0)
    out_near = pair(out_own, OUTER, False)
    qkv, out_near = lax.optimization_barrier((qkv, out_near))
    out_half = jnp.concatenate([out_own, out_near], axis=0)

    def exchange(array):
        return lax.all_to_all(
            array, AXES, split_axis=0, concat_axis=0, tiled=True, axis_index_groups=EXCHANGE
        )

    qkv, out_half = lax.optimization_barrier((exchange(qkv), out_half))
    kv_own = qkv[:, GROUP * HEAD :, :]
    kv_near = pair(kv_own, OUTER, False)
    out_half_theirs = swap(out_half)
    qkv, kv_own, kv_near, out_half, out_half_theirs = lax.optimization_barrier(
        (qkv, kv_own, kv_near, out_half, out_half_theirs)
    )
    kv_other = pair(jnp.concatenate([kv_own, kv_near], axis=0), OUTER, True)
    sums = attend(q_row, k_row, qkv, [qkv, kv_near], None)
    sums, kv_other = lax.optimization_barrier((sums, kv_other))
    out_other = pair(out_half, OUTER, True)
    attended = attend(q_row, k_row, qkv, [kv_other], sums)
    attended, out_other = lax.optimization_barrier((attended, out_other))
    attended = exchange(attended)
    return mix(
        where,
        attended.reshape(OUT_IN, TOK),
        [out_half, out_other],
        [out_half_theirs, swap(out_other)],
    )[None]


def solution(mesh):
    return jax.shard_map(
        per_device,
        mesh=mesh,
        in_specs=(
            P("dp", "sp", None),
            P(("sp", "dp"), None),
            P(("sp", "dp"), None),
            P(("sp", "dp"), None),
            P(None, ("sp", "dp")),
            P(),
            P(),
        ),
        out_specs=P("dp", "sp", None),
        check_vma=False,
    )
```

```python
import jax
import jax.numpy as jnp
import numpy as np
from jax import lax
from jax.experimental import pallas as pl
from jax.experimental.pallas import tpu as pltpu
from jax.sharding import PartitionSpec as P

GRID_W = 64
LOG2E = 1.4426950408889634
V_ROWS = 80
ATTEND_VMEM = 24 * 2**20
HEAD = 64
KV_HEADS = 4
GROUP = 4
TOK = 384
WIDE = 384
QKV = KV_HEADS * WIDE
OUT_IN = 1024
MODEL = 2048

epsilon = 1e-06
rope_base = 10000.0

AXES = ("sp", "dp")
DEVICE = np.arange(128).reshape(4, 4, 4, 2)
SHIFTS = (0, -1, 1, 2)


def lines(axis, core):
    return np.moveaxis(DEVICE[..., core], "zxy".index(axis), -1).reshape(-1, 4).tolist()


def shift_pairs(axis_of_core, step):
    pairs = []
    for core, axis in enumerate(axis_of_core):
        for line in lines(axis, core):
            pairs += [(line[i], line[(i + step) % 4]) for i in range(4)]
    return pairs


INNER = ("x", "z")
OUTER = ("z", "x")
SWAP = [(int(i), int(i) ^ 1) for i in range(128)]
EXCHANGE = lines("x", 0) + lines("z", 1)


def shift(array, axis_of_core, step):
    return lax.ppermute(array, AXES, shift_pairs(axis_of_core, step))


def pair(array, axis_of_core, far):
    pairs = []
    for core, axis in enumerate(axis_of_core):
        for line in lines(axis, core):
            pairs += [(line[i], line[3 - i if far else i ^ 1]) for i in range(4)]
    return lax.ppermute(array, AXES, pairs)


def swap(array):
    return lax.ppermute(array, AXES, SWAP)


def ring(top, bottom, axis_of_core):
    left_top = shift(top, axis_of_core, 1)
    right_bottom = shift(bottom, axis_of_core, -1)
    left_bottom = shift(bottom, axis_of_core, 1)
    right_top = shift(top, axis_of_core, -1)
    far_top = shift(left_top, axis_of_core, 1)
    far_bottom = shift(right_bottom, axis_of_core, -1)
    return left_top, left_bottom, right_top, right_bottom, far_top, far_bottom


def ring_order(at):
    return [(at + s + 4) % 4 for s in SHIFTS]


def pair_order(at):
    near = at + 1 - 2 * (at % 2)
    return [at, near, 3 - at, 3 - near]


def lay_out(where, mine, theirs, full_ref, outer_order):
    z, x, y, own_core = where
    y_at = ring_order(y)
    for pieces, core in ((mine, own_core), (theirs, 1 - own_core)):
        first = core == 0
        outer_at = outer_order(jnp.where(first, z, x))
        inner_at = ring_order(jnp.where(first, x, z))
        stack = [(p, r) for p in pieces for r in range(0, p.shape[0], 16)]
        for outer in range(4):
            for inner in range(4):
                z_at = jnp.where(first, outer_at[outer], inner_at[inner])
                x_at = jnp.where(first, inner_at[inner], outer_at[outer])
                base = (z_at * 4 + x_at) * 128 + core * 16
                for step in range(4):
                    source, row = stack[outer * 16 + inner * 4 + step]
                    at = pl.multiple_of(base + y_at[step] * 32, 16)
                    full_ref[pl.ds(at, 16), :] = source[row : row + 16, :]


def column(row):
    size = row.shape[1]
    diagonal = lax.broadcasted_iota(jnp.int32, (size, size), 0) == lax.broadcasted_iota(
        jnp.int32, (size, size), 1
    )
    return jnp.sum(jnp.where(diagonal, row, 0.0), axis=1, keepdims=True)


def project(where, tokens, mine, theirs, tables, q_gain, k_gain):
    count = len(mine)

    def kern(where_ref, tok_ref, *refs):
        table_ref, qg_ref, kg_ref, out_ref, full_ref = refs[2 * count :]
        place = [where_ref[i] for i in range(4)]
        lay_out(place, refs[:count], refs[count : 2 * count], full_ref, ring_order)
        cos_r, sin_r = table_ref[0:16, :], table_ref[16:32, :]
        cos_c, sin_c = table_ref[32:48, :], table_ref[48:64, :]
        gains = (column(qg_ref[...]), column(kg_ref[...]))
        tok = tok_ref[...]
        heads = GROUP * KV_HEADS
        for pair in range((heads + 2 * KV_HEADS) // 2):
            cols = slice(pair * 2 * HEAD, (pair + 1) * 2 * HEAD)
            if pair % 2 == 0:
                both = slice(cols.start, cols.start + 4 * HEAD)
                raw = jnp.dot(tok, full_ref[:, both], preferred_element_type=jnp.float32)
            flat = raw[:, (pair % 2) * 2 * HEAD : (pair % 2 + 1) * 2 * HEAD].T
            for i in range(2):
                head = 2 * pair + i
                v = flat[i * HEAD : (i + 1) * HEAD, :]
                if head < heads + KV_HEADS:
                    mean_sq = jnp.mean(v * v, axis=0, keepdims=True)
                    v = v * lax.rsqrt(mean_sq + epsilon) * gains[head // heads]
                    a, b, c, d = v[0:16], v[16:32], v[32:48], v[48:64]
                    v = jnp.concatenate(
                        [
                            a * cos_r - b * sin_r,
                            b * cos_r + a * sin_r,
                            c * cos_c - d * sin_c,
                            d * cos_c + c * sin_c,
                        ],
                        axis=0,
                    )
                if head < heads:
                    group, at = head // GROUP, head % GROUP
                else:
                    group, at = head % KV_HEADS, GROUP + (head - heads) // KV_HEADS
                out_ref[group, at * HEAD : (at + 1) * HEAD, :] = v.astype(jnp.bfloat16)

    return pl.pallas_call(
        kern,
        in_specs=[pl.BlockSpec(memory_space=pltpu.SMEM)]
        + [pl.BlockSpec(memory_space=pltpu.VMEM)] * (2 * count + 4),
        out_specs=pl.BlockSpec(memory_space=pltpu.VMEM),
        out_shape=jax.ShapeDtypeStruct((KV_HEADS, WIDE, TOK), jnp.bfloat16),
        scratch_shapes=[pltpu.VMEM((MODEL, QKV), jnp.bfloat16)],
        compiler_params=pltpu.CompilerParams(vmem_limit_bytes=28 * 2**20),
        cost_estimate=pl.CostEstimate(
            flops=2 * TOK * MODEL * QKV, bytes_accessed=2 * MODEL * QKV, transcendentals=0
        ),
        name="project",
    )(where, tokens, *mine, *theirs, tables, q_gain, k_gain)


def attend(q_gain, k_gain, qkv, pieces, before, last):
    keys = sum(p.shape[0] for p in pieces) * TOK
    tile = 256
    block = 512
    ahead = 2
    wide = 4 * TOK
    more = before is not None

    def kern(qg_ref, kg_ref, q_ref, *refs):
        sources = refs[: len(pieces)]
        rest = refs[len(pieces) :]
        if more:
            acc_in, top_in = rest[:2]
            rest = rest[2:]
        if last:
            o_ref, k_ref, v_ref = rest
        else:
            acc_out, top_out, k_ref, v_ref = rest

        @pl.when(pl.program_id(0) == 0)
        def _():
            at = 0
            for source in sources:
                for i in range(source.shape[0]):
                    k = source[i, 0:HEAD, :]
                    k_ref[at : at + TOK, :] = jnp.concatenate([k, k], axis=0).T
                    v_ref[0:HEAD, at : at + TOK] = source[i, HEAD : 2 * HEAD, :]
                    at += TOK
            row = lax.broadcasted_iota(jnp.int32, (V_ROWS - HEAD, keys), 0)
            v_ref[HEAD:, :] = jnp.where(row == 0, 1.0, 0.0).astype(jnp.bfloat16)

        q = jnp.concatenate([q_ref[i] for i in range(4)], axis=1)
        limit = 8.0 * jnp.max(jnp.abs(qg_ref[...])) * jnp.max(jnp.abs(kg_ref[...]))

        def finish(acc, top):
            if last:
                done = (acc[:HEAD] / acc[HEAD : HEAD + 1]).astype(jnp.bfloat16)
                for i in range(4):
                    o_ref[i] = done[:, i * TOK : (i + 1) * TOK]
            else:
                acc_out[0] = acc
                top_out[0] = top

        @pl.when(limit <= 60.0)
        def _():
            scaled = q.astype(jnp.float32) * (0.125 * LOG2E)
            high = scaled.astype(jnp.bfloat16)
            low = (scaled - high.astype(jnp.float32)).astype(jnp.bfloat16)
            q2 = jnp.concatenate([high, low], axis=0)
            work = [(b, u) for b in range(0, wide, block) for u in range(0, keys, tile)]

            def score(item):
                b, u = item
                return jnp.dot(
                    k_ref[u : u + tile, :], q2[:, b : b + block], preferred_element_type=jnp.float32
                )

            waiting = [score(item) for item in work[:ahead]]
            done = []
            for n, (b, u) in enumerate(work):
                if n + ahead < len(work):
                    waiting.append(score(work[n + ahead]))
                if u == 0 and more:
                    acc = acc_in[0, :, b : b + block]
                elif u == 0:
                    acc = jnp.zeros((V_ROWS, block), jnp.float32)
                weights = jnp.exp2(waiting.pop(0)).astype(jnp.bfloat16)
                acc = acc + jnp.dot(
                    v_ref[:, u : u + tile], weights, preferred_element_type=jnp.float32
                )
                if u + tile == keys:
                    done.append(acc)
            acc = jnp.concatenate(done, axis=1)
            finish(acc, jnp.zeros((8, wide), jnp.float32))

        @pl.when(jnp.logical_not(limit <= 60.0))
        def _():
            step_rows = 512

            def step(u, carry):
                top, acc = carry
                rows = pl.ds(pl.multiple_of(u * step_rows, step_rows), step_rows)
                scores = (
                    jnp.dot(k_ref[rows, :HEAD], q, preferred_element_type=jnp.float32) * 0.125
                )
                new_top = jnp.maximum(top, jnp.max(scores, axis=0, keepdims=True))
                weights = jnp.exp(scores - new_top).astype(jnp.bfloat16)
                part = jnp.dot(v_ref[:, rows], weights, preferred_element_type=jnp.float32)
                return new_top, acc * jnp.exp(top - new_top) + part

            if more:
                start = (top_in[0, 0:1, :], acc_in[0])
            else:
                start = (
                    jnp.full((1, wide), -1e30, jnp.float32),
                    jnp.zeros((V_ROWS, wide), jnp.float32),
                )
            top, acc = lax.fori_loop(0, keys // step_rows, step, start)
            finish(acc, jnp.broadcast_to(top, (8, wide)))

    def whole(array, at):
        return pl.BlockSpec((array.shape[0], 2 * HEAD, TOK), lambda h: (0, at, 0))

    sums = [
        pl.BlockSpec((1, V_ROWS, wide), lambda h: (h, 0, 0)),
        pl.BlockSpec((1, 8, wide), lambda h: (h, 0, 0)),
    ]
    gain = pl.BlockSpec((1, HEAD), lambda h: (0, 0))
    return pl.pallas_call(
        kern,
        grid=(GROUP,),
        in_specs=[
            gain,
            gain,
            pl.BlockSpec((4, HEAD, TOK), lambda h: (0, h, 0)),
            *[whole(p, 0 if p.shape[1] == 2 * HEAD else 2) for p in pieces],
            *(sums if more else []),
        ],
        out_specs=pl.BlockSpec((4, HEAD, TOK), lambda h: (0, h, 0)) if last else sums,
        out_shape=jax.ShapeDtypeStruct((4, GROUP * HEAD, TOK), jnp.bfloat16)
        if last
        else [
            jax.ShapeDtypeStruct((GROUP, V_ROWS, wide), jnp.float32),
            jax.ShapeDtypeStruct((GROUP, 8, wide), jnp.float32),
        ],
        scratch_shapes=[
            pltpu.VMEM((keys, 2 * HEAD), jnp.bfloat16),
            pltpu.VMEM((V_ROWS, keys), jnp.bfloat16),
        ],
        compiler_params=pltpu.CompilerParams(vmem_limit_bytes=ATTEND_VMEM),
        cost_estimate=pl.CostEstimate(
            flops=16 * keys * wide * 256 * 2,
            bytes_accessed=2 * keys * 2 * HEAD,
            transcendentals=GROUP * keys * wide,
        ),
        name="attend_last" if last else "attend_more" if more else "attend_first",
    )(q_gain, k_gain, qkv, *pieces, *(before or []))


def mix(where, attended, mine, theirs):
    count = len(mine)

    def kern(where_ref, att_ref, *refs):
        out_ref, full_ref = refs[2 * count :]
        place = [where_ref[i] for i in range(4)]
        lay_out(place, refs[:count], refs[count : 2 * count], full_ref, pair_order)
        rows = att_ref[...].T
        out_ref[...] = lax.dot_general(
            rows, full_ref[...], (((1,), (1,)), ((), ())), preferred_element_type=jnp.float32
        ).astype(jnp.bfloat16)

    def piece(array):
        return pl.BlockSpec(array.shape, lambda: (0, 0))

    return pl.pallas_call(
        kern,
        in_specs=[
            pl.BlockSpec(memory_space=pltpu.SMEM),
            pl.BlockSpec((OUT_IN, TOK), lambda: (0, 0)),
            *[piece(a) for a in mine],
            *[piece(a) for a in theirs],
        ],
        out_specs=pl.BlockSpec((TOK, MODEL), lambda: (0, 0)),
        out_shape=jax.ShapeDtypeStruct((TOK, MODEL), jnp.bfloat16),
        scratch_shapes=[pltpu.VMEM((MODEL, OUT_IN), jnp.bfloat16)],
        compiler_params=pltpu.CompilerParams(vmem_limit_bytes=24 * 2**20),
        cost_estimate=pl.CostEstimate(
            flops=2 * TOK * MODEL * OUT_IN, bytes_accessed=2 * MODEL * OUT_IN, transcendentals=0
        ),
        name="mix",
    )(where, attended, *mine, *theirs)


def rotation_tables(offset):
    quarter = HEAD // 4
    positions = jnp.arange(TOK, dtype=jnp.int32) + offset
    frequency = rope_base ** (-jnp.arange(quarter, dtype=jnp.float32) / quarter)
    parts = []
    for coords in (positions // GRID_W, positions % GRID_W):
        angles = coords.astype(jnp.float32)[None, :] * frequency[:, None]
        parts += [jnp.cos(angles), jnp.sin(angles)]
    return jnp.concatenate(parts, axis=0)


def per_device(tokens, q_weight, k_weight, v_weight, out_weight, q_gain, k_gain):
    sp = lax.axis_index("sp")
    dp = lax.axis_index("dp")
    where = jnp.stack([sp // 4, sp % 4, dp // 2, dp % 2]).astype(jnp.int32)
    tables = rotation_tables(sp * TOK)
    q_row = q_gain.reshape(1, HEAD)
    k_row = k_gain.reshape(1, HEAD)

    own = jnp.concatenate([q_weight, k_weight, v_weight, out_weight.T], axis=1)
    block = jnp.concatenate([own, *[shift(own, ("y", "y"), -s) for s in SHIFTS[1:]]], axis=0)
    left = shift(block, INNER, 1)
    right = shift(block, INNER, -1)
    middle = block.shape[0] // 2
    far_top = shift(left[:middle], INNER, 1)
    far_bottom = shift(right[middle:], INNER, -1)
    half = jnp.concatenate([block, left], axis=0)
    other = jnp.concatenate([right, far_top, far_bottom], axis=0)
    tables, where, half, other = lax.optimization_barrier((tables, where, half, other))

    in_mine = [half[:, :QKV], other[:, :QKV]]
    in_mine += ring(*in_mine, OUTER)
    in_theirs = [swap(a) for a in in_mine]
    qkv = project(where, tokens[0], in_mine, in_theirs, tables, q_row, k_row)

    out_own = jnp.concatenate([half[:, QKV:], other[:, QKV:]], axis=0)
    out_near = pair(out_own, OUTER, False)

    def exchange(array):
        return lax.all_to_all(
            array, AXES, split_axis=0, concat_axis=0, tiled=True, axis_index_groups=EXCHANGE
        )

    qkv, out_near = lax.optimization_barrier((exchange(qkv), out_near))
    out_half = jnp.concatenate([out_own, out_near], axis=0)
    kv_own = qkv[:, GROUP * HEAD :, :]
    kv_near = pair(kv_own, OUTER, False)
    out_half_theirs = swap(out_half)
    sums = attend(q_row, k_row, qkv, [qkv], None, False)
    sums, kv_own, kv_near, out_half, out_half_theirs = lax.optimization_barrier(
        (sums, kv_own, kv_near, out_half, out_half_theirs)
    )
    kv_other = pair(jnp.concatenate([kv_own, kv_near], axis=0), OUTER, True)
    out_other = pair(out_half, OUTER, True)
    sums = attend(q_row, k_row, qkv, [kv_near], sums, False)
    sums, kv_other = lax.optimization_barrier((sums, kv_other))
    attended = attend(q_row, k_row, qkv, [kv_other], sums, True)
    attended, out_other = lax.optimization_barrier((attended, out_other))
    attended = exchange(attended)
    return mix(
        where,
        attended.reshape(OUT_IN, TOK),
        [out_half, out_other],
        [out_half_theirs, swap(out_other)],
    )[None]


def solution(mesh):
    return jax.shard_map(
        per_device,
        mesh=mesh,
        in_specs=(
            P("dp", "sp", None),
            P(("sp", "dp"), None),
            P(("sp", "dp"), None),
            P(("sp", "dp"), None),
            P(None, ("sp", "dp")),
            P(),
            P(),
        ),
        out_specs=P("dp", "sp", None),
        check_vma=False,
    )
```

```python
import jax
import jax.numpy as jnp
import numpy as np
from jax import lax
from jax.experimental import pallas as pl
from jax.experimental.pallas import tpu as pltpu
from jax.sharding import PartitionSpec as P

GRID_W = 64
LOG2E = 1.4426950408889634
V_ROWS = 80
ATTEND_VMEM = 24 * 2**20
HEAD = 64
KV_HEADS = 4
GROUP = 4
TOK = 384
WIDE = 384
QKV = KV_HEADS * WIDE
OUT_IN = 1024
MODEL = 2048

epsilon = 1e-06
rope_base = 10000.0

AXES = ("sp", "dp")
DEVICE = np.arange(128).reshape(4, 4, 4, 2)
SHIFTS = (0, -1, 1, 2)


def lines(axis, core):
    return np.moveaxis(DEVICE[..., core], "zxy".index(axis), -1).reshape(-1, 4).tolist()


def shift_pairs(axis_of_core, step):
    pairs = []
    for core, axis in enumerate(axis_of_core):
        for line in lines(axis, core):
            pairs += [(line[i], line[(i + step) % 4]) for i in range(4)]
    return pairs


INNER = ("x", "z")
OUTER = ("z", "x")
SWAP = [(int(i), int(i) ^ 1) for i in range(128)]
EXCHANGE = lines("x", 0) + lines("z", 1)


def shift(array, axis_of_core, step):
    return lax.ppermute(array, AXES, shift_pairs(axis_of_core, step))


def pair(array, axis_of_core, far):
    pairs = []
    for core, axis in enumerate(axis_of_core):
        for line in lines(axis, core):
            pairs += [(line[i], line[3 - i if far else i ^ 1]) for i in range(4)]
    return lax.ppermute(array, AXES, pairs)


def swap(array):
    return lax.ppermute(array, AXES, SWAP)


def ring(top, bottom, axis_of_core):
    left_top = shift(top, axis_of_core, 1)
    right_bottom = shift(bottom, axis_of_core, -1)
    left_bottom = shift(bottom, axis_of_core, 1)
    right_top = shift(top, axis_of_core, -1)
    far_top = shift(left_top, axis_of_core, 1)
    far_bottom = shift(right_bottom, axis_of_core, -1)
    return left_top, left_bottom, right_top, right_bottom, far_top, far_bottom


def ring_order(at):
    return [(at + s + 4) % 4 for s in SHIFTS]


def pair_order(at):
    near = at + 1 - 2 * (at % 2)
    return [at, near, 3 - at, 3 - near]


def lay_out(where, mine, theirs, full_ref, outer_order):
    z, x, y, own_core = where
    y_at = ring_order(y)
    for pieces, core in ((mine, own_core), (theirs, 1 - own_core)):
        first = core == 0
        outer_at = outer_order(jnp.where(first, z, x))
        inner_at = ring_order(jnp.where(first, x, z))
        stack = [(p, r) for p in pieces for r in range(0, p.shape[0], 16)]
        for outer in range(4):
            for inner in range(4):
                z_at = jnp.where(first, outer_at[outer], inner_at[inner])
                x_at = jnp.where(first, inner_at[inner], outer_at[outer])
                base = (z_at * 4 + x_at) * 128 + core * 16
                for step in range(4):
                    source, row = stack[outer * 16 + inner * 4 + step]
                    at = pl.multiple_of(base + y_at[step] * 32, 16)
                    full_ref[pl.ds(at, 16), :] = source[row : row + 16, :]


def column(row):
    size = row.shape[1]
    diagonal = lax.broadcasted_iota(jnp.int32, (size, size), 0) == lax.broadcasted_iota(
        jnp.int32, (size, size), 1
    )
    return jnp.sum(jnp.where(diagonal, row, 0.0), axis=1, keepdims=True)


def project(where, tokens, mine, theirs, tables, q_gain, k_gain):
    count = len(mine)

    def kern(where_ref, tok_ref, *refs):
        table_ref, qg_ref, kg_ref, out_ref, full_ref = refs[2 * count :]
        place = [where_ref[i] for i in range(4)]
        lay_out(place, refs[:count], refs[count : 2 * count], full_ref, ring_order)
        cos_r, sin_r = table_ref[0:16, :], table_ref[16:32, :]
        cos_c, sin_c = table_ref[32:48, :], table_ref[48:64, :]
        gains = (column(qg_ref[...]), column(kg_ref[...]))
        tok = tok_ref[...]
        heads = GROUP * KV_HEADS
        for pair in range((heads + 2 * KV_HEADS) // 2):
            cols = slice(pair * 2 * HEAD, (pair + 1) * 2 * HEAD)
            if pair % 2 == 0:
                both = slice(cols.start, cols.start + 4 * HEAD)
                raw = jnp.dot(tok, full_ref[:, both], preferred_element_type=jnp.float32)
            flat = raw[:, (pair % 2) * 2 * HEAD : (pair % 2 + 1) * 2 * HEAD].T
            for i in range(2):
                head = 2 * pair + i
                v = flat[i * HEAD : (i + 1) * HEAD, :]
                if head < heads + KV_HEADS:
                    mean_sq = jnp.mean(v * v, axis=0, keepdims=True)
                    v = v * lax.rsqrt(mean_sq + epsilon) * gains[head // heads]
                    a, b, c, d = v[0:16], v[16:32], v[32:48], v[48:64]
                    v = jnp.concatenate(
                        [
                            a * cos_r - b * sin_r,
                            b * cos_r + a * sin_r,
                            c * cos_c - d * sin_c,
                            d * cos_c + c * sin_c,
                        ],
                        axis=0,
                    )
                if head < heads:
                    group, at = head // GROUP, head % GROUP
                else:
                    group, at = head % KV_HEADS, GROUP + (head - heads) // KV_HEADS
                out_ref[group, at * HEAD : (at + 1) * HEAD, :] = v.astype(jnp.bfloat16)

    return pl.pallas_call(
        kern,
        in_specs=[pl.BlockSpec(memory_space=pltpu.SMEM)]
        + [pl.BlockSpec(memory_space=pltpu.VMEM)] * (2 * count + 4),
        out_specs=pl.BlockSpec(memory_space=pltpu.VMEM),
        out_shape=jax.ShapeDtypeStruct((KV_HEADS, WIDE, TOK), jnp.bfloat16),
        scratch_shapes=[pltpu.VMEM((MODEL, QKV), jnp.bfloat16)],
        compiler_params=pltpu.CompilerParams(vmem_limit_bytes=28 * 2**20),
        cost_estimate=pl.CostEstimate(
            flops=2 * TOK * MODEL * QKV, bytes_accessed=2 * MODEL * QKV, transcendentals=0
        ),
        name="project",
    )(where, tokens, *mine, *theirs, tables, q_gain, k_gain)


def attend(place, q_gain, k_gain, qkv, pieces, before, last):
    keys = sum(p.shape[0] for p in pieces) * TOK
    places = place.shape[0]
    tile = 256
    block = 512
    ahead = 2
    wide = GROUP * TOK
    more = before is not None

    def kern(place_ref, qg_ref, kg_ref, q_ref, *refs):
        sources = refs[: len(pieces)]
        rest = refs[len(pieces) :]
        if more:
            acc_in, top_in = rest[:2]
            rest = rest[2:]
        *outs, k_ref, v_ref = rest

        @pl.when(pl.program_id(0) == 0)
        def _():
            at = 0
            for source in sources:
                for i in range(source.shape[0]):
                    k = source[i, 0:HEAD, :]
                    k_ref[at : at + TOK, :] = jnp.concatenate([k, k], axis=0).T
                    v_ref[0:HEAD, at : at + TOK] = source[i, HEAD : 2 * HEAD, :]
                    at += TOK
            row = lax.broadcasted_iota(jnp.int32, (V_ROWS - HEAD, keys), 0)
            v_ref[HEAD:, :] = jnp.where(row == 0, 1.0, 0.0).astype(jnp.bfloat16)

        q = jnp.concatenate([q_ref[0, h * HEAD : (h + 1) * HEAD, :] for h in range(GROUP)], axis=1)
        limit = 8.0 * jnp.max(jnp.abs(qg_ref[...])) * jnp.max(jnp.abs(kg_ref[...]))

        def finish(acc, top):
            if not last:
                outs[0][0] = acc
                outs[1][0] = top
                return
            result = (acc[:HEAD] / acc[HEAD : HEAD + 1]).astype(jnp.bfloat16)
            for n in range(places):

                @pl.when(pl.program_id(0) == n)
                def _():
                    for h in range(GROUP):
                        outs[n][h * HEAD : (h + 1) * HEAD, :] = result[:, h * TOK : (h + 1) * TOK]

        @pl.when(limit <= 60.0)
        def _():
            scaled = q.astype(jnp.float32) * (0.125 * LOG2E)
            high = scaled.astype(jnp.bfloat16)
            low = (scaled - high.astype(jnp.float32)).astype(jnp.bfloat16)
            q2 = jnp.concatenate([high, low], axis=0)
            work = [(b, u) for b in range(0, wide, block) for u in range(0, keys, tile)]

            def score(item):
                b, u = item
                return jnp.dot(
                    k_ref[u : u + tile, :], q2[:, b : b + block], preferred_element_type=jnp.float32
                )

            waiting = [score(item) for item in work[:ahead]]
            done = []
            for n, (b, u) in enumerate(work):
                if n + ahead < len(work):
                    waiting.append(score(work[n + ahead]))
                if u == 0 and more:
                    acc = acc_in[0, :, b : b + block]
                elif u == 0:
                    acc = jnp.zeros((V_ROWS, block), jnp.float32)
                weights = jnp.exp2(waiting.pop(0)).astype(jnp.bfloat16)
                acc = acc + jnp.dot(
                    v_ref[:, u : u + tile], weights, preferred_element_type=jnp.float32
                )
                if u + tile == keys:
                    done.append(acc)
            finish(jnp.concatenate(done, axis=1), jnp.zeros((8, wide), jnp.float32))

        @pl.when(jnp.logical_not(limit <= 60.0))
        def _():
            step_rows = 512

            def step(u, carry):
                top, acc = carry
                rows = pl.ds(pl.multiple_of(u * step_rows, step_rows), step_rows)
                scores = (
                    jnp.dot(k_ref[rows, :HEAD], q, preferred_element_type=jnp.float32) * 0.125
                )
                new_top = jnp.maximum(top, jnp.max(scores, axis=0, keepdims=True))
                weights = jnp.exp(scores - new_top).astype(jnp.bfloat16)
                part = jnp.dot(v_ref[:, rows], weights, preferred_element_type=jnp.float32)
                return new_top, acc * jnp.exp(top - new_top) + part

            if more:
                start = (top_in[0, 0:1, :], acc_in[0])
            else:
                start = (
                    jnp.full((1, wide), -1e30, jnp.float32),
                    jnp.zeros((V_ROWS, wide), jnp.float32),
                )
            top, acc = lax.fori_loop(0, keys // step_rows, step, start)
            finish(acc, jnp.broadcast_to(top, (8, wide)))

    def whole(array, at):
        return pl.BlockSpec((array.shape[0], 2 * HEAD, TOK), lambda n, place: (0, at, 0))

    sums = [
        pl.BlockSpec((1, V_ROWS, wide), lambda n, place: (place[n], 0, 0)),
        pl.BlockSpec((1, 8, wide), lambda n, place: (place[n], 0, 0)),
    ]
    gain = pl.BlockSpec((1, HEAD), lambda n, place: (0, 0))
    result = pl.BlockSpec((GROUP * HEAD, TOK), lambda n, place: (0, 0))
    return pl.pallas_call(
        kern,
        grid_spec=pltpu.PrefetchScalarGridSpec(
            num_scalar_prefetch=1,
            grid=(places,),
            in_specs=[
                gain,
                gain,
                pl.BlockSpec((1, GROUP * HEAD, TOK), lambda n, place: (place[n], 0, 0)),
                *[whole(p, 0 if p.shape[1] == 2 * HEAD else 2) for p in pieces],
                *(sums if more else []),
            ],
            out_specs=[result] * places if last else sums,
            scratch_shapes=[
                pltpu.VMEM((keys, 2 * HEAD), jnp.bfloat16),
                pltpu.VMEM((V_ROWS, keys), jnp.bfloat16),
            ],
        ),
        out_shape=[jax.ShapeDtypeStruct((GROUP * HEAD, TOK), jnp.bfloat16)] * places
        if last
        else [
            jax.ShapeDtypeStruct((4, V_ROWS, wide), jnp.float32),
            jax.ShapeDtypeStruct((4, 8, wide), jnp.float32),
        ],
        compiler_params=pltpu.CompilerParams(vmem_limit_bytes=ATTEND_VMEM),
        cost_estimate=pl.CostEstimate(
            flops=4 * places * keys * wide * 256 * 2,
            bytes_accessed=2 * keys * 2 * HEAD,
            transcendentals=places * keys * wide,
        ),
    )(place, q_gain, k_gain, qkv, *pieces, *(before or []))


def mix(where, attended, mine, theirs):
    count = len(mine)

    def kern(where_ref, *refs):
        heads = refs[:4]
        refs = refs[4:]
        out_ref, full_ref, att_ref = refs[2 * count :]
        place = [where_ref[i] for i in range(4)]
        lay_out(place, refs[:count], refs[count : 2 * count], full_ref, pair_order)
        groups = ring_order(jnp.where(place[3] == 0, place[1], place[0]))
        for group, source in zip(groups, heads):
            at = pl.multiple_of(group * GROUP * HEAD, GROUP * HEAD)
            att_ref[pl.ds(at, GROUP * HEAD), :] = source[...]
        rows = att_ref[...].T
        out_ref[...] = lax.dot_general(
            rows, full_ref[...], (((1,), (1,)), ((), ())), preferred_element_type=jnp.float32
        ).astype(jnp.bfloat16)

    def piece(array):
        return pl.BlockSpec(array.shape, lambda: (0, 0))

    return pl.pallas_call(
        kern,
        in_specs=[
            pl.BlockSpec(memory_space=pltpu.SMEM),
            *[piece(a) for a in attended],
            *[piece(a) for a in mine],
            *[piece(a) for a in theirs],
        ],
        out_specs=pl.BlockSpec((TOK, MODEL), lambda: (0, 0)),
        out_shape=jax.ShapeDtypeStruct((TOK, MODEL), jnp.bfloat16),
        scratch_shapes=[
            pltpu.VMEM((MODEL, OUT_IN), jnp.bfloat16),
            pltpu.VMEM((OUT_IN, TOK), jnp.bfloat16),
        ],
        compiler_params=pltpu.CompilerParams(vmem_limit_bytes=24 * 2**20),
        cost_estimate=pl.CostEstimate(
            flops=2 * TOK * MODEL * OUT_IN, bytes_accessed=2 * MODEL * OUT_IN, transcendentals=0
        ),
        name="mix",
    )(where, *attended, *mine, *theirs)


def rotation_tables(offset):
    quarter = HEAD // 4
    positions = jnp.arange(TOK, dtype=jnp.int32) + offset
    frequency = rope_base ** (-jnp.arange(quarter, dtype=jnp.float32) / quarter)
    parts = []
    for coords in (positions // GRID_W, positions % GRID_W):
        angles = coords.astype(jnp.float32)[None, :] * frequency[:, None]
        parts += [jnp.cos(angles), jnp.sin(angles)]
    return jnp.concatenate(parts, axis=0)


def per_device(tokens, q_weight, k_weight, v_weight, out_weight, q_gain, k_gain):
    sp = lax.axis_index("sp")
    dp = lax.axis_index("dp")
    where = jnp.stack([sp // 4, sp % 4, dp // 2, dp % 2]).astype(jnp.int32)
    tables = rotation_tables(sp * TOK)
    q_row = q_gain.reshape(1, HEAD)
    k_row = k_gain.reshape(1, HEAD)

    own = jnp.concatenate([q_weight, k_weight, v_weight, out_weight.T], axis=1)
    block = jnp.concatenate([own, *[shift(own, ("y", "y"), -s) for s in SHIFTS[1:]]], axis=0)
    left = shift(block, INNER, 1)
    right = shift(block, INNER, -1)
    middle = block.shape[0] // 2
    far_top = shift(left[:middle], INNER, 1)
    far_bottom = shift(right[middle:], INNER, -1)
    half = jnp.concatenate([block, left], axis=0)
    other = jnp.concatenate([right, far_top, far_bottom], axis=0)
    tables, where, half, other = lax.optimization_barrier((tables, where, half, other))

    in_mine = [half[:, :QKV], other[:, :QKV]]
    in_mine += ring(*in_mine, OUTER)
    in_theirs = [swap(a) for a in in_mine]
    qkv = project(where, tokens[0], in_mine, in_theirs, tables, q_row, k_row)

    out_own = jnp.concatenate([half[:, QKV:], other[:, QKV:]], axis=0)
    qkv, out_own = lax.optimization_barrier(
        (
            lax.all_to_all(
                qkv, AXES, split_axis=0, concat_axis=0, tiled=True, axis_index_groups=EXCHANGE
            ),
            out_own,
        )
    )
    every = jnp.arange(4, dtype=jnp.int32)
    here = jnp.where(dp % 2 == 0, sp % 4, sp // 4).astype(jnp.int32)
    away = jnp.stack(ring_order(here)[1:])
    kv_own = qkv[:, GROUP * HEAD :, :]
    kv_near = pair(kv_own, OUTER, False)
    out_near = pair(out_own, OUTER, False)
    sums = attend(every, q_row, k_row, qkv, [qkv], None, False)
    sums, kv_own, kv_near = lax.optimization_barrier((sums, kv_own, kv_near))
    kv_other = pair(jnp.concatenate([kv_own, kv_near], axis=0), OUTER, True)
    sums = attend(every, q_row, k_row, qkv, [kv_near], sums, False)
    sums, kv_other, out_near = lax.optimization_barrier((sums, kv_other, out_near))
    out_half = jnp.concatenate([out_own, out_near], axis=0)
    out_other = pair(out_half, OUTER, True)
    out_half_theirs = swap(out_half)
    behind, ahead, across = attend(away, q_row, k_row, qkv, [kv_other], sums, True)
    sums, kv_other, behind, ahead, across, out_half_theirs = lax.optimization_barrier(
        (sums, kv_other, behind, ahead, across, out_half_theirs)
    )
    across = shift(across, INNER, 2)
    ahead = shift(ahead, INNER, 1)
    behind = shift(behind, INNER, -1)
    (own,) = attend(here.reshape(1), q_row, k_row, qkv, [kv_other], sums, True)
    own, out_other = lax.optimization_barrier((own, out_other))
    out_other_theirs = swap(out_other)
    return mix(
        where, [own, ahead, behind, across], [out_half, out_other], [out_half_theirs, out_other_theirs]
    )[None]


def solution(mesh):
    return jax.shard_map(
        per_device,
        mesh=mesh,
        in_specs=(
            P("dp", "sp", None),
            P(("sp", "dp"), None),
            P(("sp", "dp"), None),
            P(("sp", "dp"), None),
            P(None, ("sp", "dp")),
            P(),
            P(),
        ),
        out_specs=P("dp", "sp", None),
        check_vma=False,
    )
```

```python
import jax
import jax.numpy as jnp
import numpy as np
from jax import lax
from jax.experimental import pallas as pl
from jax.experimental.pallas import tpu as pltpu
from jax.sharding import PartitionSpec as P

GRID_W = 64
LOG2E = 1.4426950408889634
V_ROWS = 80
ATTEND_VMEM = 24 * 2**20
HEAD = 64
KV_HEADS = 4
GROUP = 4
TOK = 384
WIDE = 384
QKV = KV_HEADS * WIDE
OUT_IN = 1024
MODEL = 2048

epsilon = 1e-06
rope_base = 10000.0

AXES = ("sp", "dp")
DEVICE = np.arange(128).reshape(4, 4, 4, 2)
SHIFTS = (0, -1, 1, 2)


def lines(axis, core):
    return np.moveaxis(DEVICE[..., core], "zxy".index(axis), -1).reshape(-1, 4).tolist()


def shift_pairs(axis_of_core, step):
    pairs = []
    for core, axis in enumerate(axis_of_core):
        for line in lines(axis, core):
            pairs += [(line[i], line[(i + step) % 4]) for i in range(4)]
    return pairs


INNER = ("x", "z")
OUTER = ("z", "x")
SWAP = [(int(i), int(i) ^ 1) for i in range(128)]
EXCHANGE = lines("x", 0) + lines("z", 1)


def shift(array, axis_of_core, step):
    return lax.ppermute(array, AXES, shift_pairs(axis_of_core, step))


def pair(array, axis_of_core, far):
    pairs = []
    for core, axis in enumerate(axis_of_core):
        for line in lines(axis, core):
            pairs += [(line[i], line[3 - i if far else i ^ 1]) for i in range(4)]
    return lax.ppermute(array, AXES, pairs)


def swap(array):
    return lax.ppermute(array, AXES, SWAP)


def ring(top, bottom, axis_of_core):
    left_top = shift(top, axis_of_core, 1)
    right_bottom = shift(bottom, axis_of_core, -1)
    left_bottom = shift(bottom, axis_of_core, 1)
    right_top = shift(top, axis_of_core, -1)
    far_top = shift(left_top, axis_of_core, 1)
    far_bottom = shift(right_bottom, axis_of_core, -1)
    return left_top, left_bottom, right_top, right_bottom, far_top, far_bottom


def ring_order(at):
    return [(at + s + 4) % 4 for s in SHIFTS]


def pair_order(at):
    near = at + 1 - 2 * (at % 2)
    return [at, near, 3 - at, 3 - near]


def lay_out(where, mine, theirs, full_ref, outer_order):
    z, x, y, own_core = where
    y_at = ring_order(y)
    for pieces, core in ((mine, own_core), (theirs, 1 - own_core)):
        first = core == 0
        outer_at = outer_order(jnp.where(first, z, x))
        inner_at = ring_order(jnp.where(first, x, z))
        stack = [(p, r) for p in pieces for r in range(0, p.shape[0], 16)]
        for outer in range(4):
            for inner in range(4):
                z_at = jnp.where(first, outer_at[outer], inner_at[inner])
                x_at = jnp.where(first, inner_at[inner], outer_at[outer])
                base = (z_at * 4 + x_at) * 128 + core * 16
                for step in range(4):
                    source, row = stack[outer * 16 + inner * 4 + step]
                    at = pl.multiple_of(base + y_at[step] * 32, 16)
                    full_ref[pl.ds(at, 16), :] = source[row : row + 16, :]


def column(row):
    size = row.shape[1]
    diagonal = lax.broadcasted_iota(jnp.int32, (size, size), 0) == lax.broadcasted_iota(
        jnp.int32, (size, size), 1
    )
    return jnp.sum(jnp.where(diagonal, row, 0.0), axis=1, keepdims=True)


def project(where, tokens, mine, theirs, tables, q_gain, k_gain):
    count = len(mine)

    def kern(where_ref, tok_ref, *refs):
        table_ref, qg_ref, kg_ref, out_ref, full_ref = refs[2 * count :]
        place = [where_ref[i] for i in range(4)]
        lay_out(place, refs[:count], refs[count : 2 * count], full_ref, ring_order)
        cos_r, sin_r = table_ref[0:16, :], table_ref[16:32, :]
        cos_c, sin_c = table_ref[32:48, :], table_ref[48:64, :]
        gains = (column(qg_ref[...]), column(kg_ref[...]))
        tok = tok_ref[...]
        heads = GROUP * KV_HEADS
        for pair in range((heads + 2 * KV_HEADS) // 2):
            cols = slice(pair * 2 * HEAD, (pair + 1) * 2 * HEAD)
            if pair % 2 == 0:
                both = slice(cols.start, cols.start + 4 * HEAD)
                raw = jnp.dot(tok, full_ref[:, both], preferred_element_type=jnp.float32)
            flat = raw[:, (pair % 2) * 2 * HEAD : (pair % 2 + 1) * 2 * HEAD].T
            for i in range(2):
                head = 2 * pair + i
                v = flat[i * HEAD : (i + 1) * HEAD, :]
                if head < heads + KV_HEADS:
                    mean_sq = jnp.mean(v * v, axis=0, keepdims=True)
                    v = v * lax.rsqrt(mean_sq + epsilon) * gains[head // heads]
                    a, b, c, d = v[0:16], v[16:32], v[32:48], v[48:64]
                    v = jnp.concatenate(
                        [
                            a * cos_r - b * sin_r,
                            b * cos_r + a * sin_r,
                            c * cos_c - d * sin_c,
                            d * cos_c + c * sin_c,
                        ],
                        axis=0,
                    )
                if head < heads:
                    group, at = head // GROUP, head % GROUP
                else:
                    group, at = head % KV_HEADS, GROUP + (head - heads) // KV_HEADS
                out_ref[group, at * HEAD : (at + 1) * HEAD, :] = v.astype(jnp.bfloat16)

    return pl.pallas_call(
        kern,
        in_specs=[pl.BlockSpec(memory_space=pltpu.SMEM)]
        + [pl.BlockSpec(memory_space=pltpu.VMEM)] * (2 * count + 4),
        out_specs=pl.BlockSpec(memory_space=pltpu.VMEM),
        out_shape=jax.ShapeDtypeStruct((KV_HEADS, WIDE, TOK), jnp.bfloat16),
        scratch_shapes=[pltpu.VMEM((MODEL, QKV), jnp.bfloat16)],
        compiler_params=pltpu.CompilerParams(vmem_limit_bytes=28 * 2**20),
        cost_estimate=pl.CostEstimate(
            flops=2 * TOK * MODEL * QKV, bytes_accessed=2 * MODEL * QKV, transcendentals=0
        ),
        name="project",
    )(where, tokens, *mine, *theirs, tables, q_gain, k_gain)


def attend(place, q_gain, k_gain, qkv, pieces, before, last):
    keys = sum(p.shape[0] for p in pieces) * TOK
    places = place.shape[0]
    tile = 256
    block = 512
    ahead = 2
    wide = GROUP * TOK
    more = before is not None

    def kern(place_ref, qg_ref, kg_ref, q_ref, *refs):
        sources = refs[: len(pieces)]
        rest = refs[len(pieces) :]
        if more:
            acc_in, top_in = rest[:2]
            rest = rest[2:]
        *outs, k_ref, v_ref = rest

        @pl.when(pl.program_id(0) == 0)
        def _():
            at = 0
            for source in sources:
                for i in range(source.shape[0]):
                    k = source[i, 0:HEAD, :]
                    k_ref[at : at + TOK, :] = jnp.concatenate([k, k], axis=0).T
                    v_ref[0:HEAD, at : at + TOK] = source[i, HEAD : 2 * HEAD, :]
                    at += TOK
            row = lax.broadcasted_iota(jnp.int32, (V_ROWS - HEAD, keys), 0)
            v_ref[HEAD:, :] = jnp.where(row == 0, 1.0, 0.0).astype(jnp.bfloat16)

        q = jnp.concatenate([q_ref[0, h * HEAD : (h + 1) * HEAD, :] for h in range(GROUP)], axis=1)
        limit = 8.0 * jnp.max(jnp.abs(qg_ref[...])) * jnp.max(jnp.abs(kg_ref[...]))

        def finish(acc, top):
            if not last:
                outs[0][0] = acc
                outs[1][0] = top
                return
            result = (acc[:HEAD] / acc[HEAD : HEAD + 1]).astype(jnp.bfloat16)
            for n in range(places):

                @pl.when(pl.program_id(0) == n)
                def _():
                    for h in range(GROUP):
                        outs[n][h * HEAD : (h + 1) * HEAD, :] = result[:, h * TOK : (h + 1) * TOK]

        @pl.when(limit <= 60.0)
        def _():
            scaled = q.astype(jnp.float32) * (0.125 * LOG2E)
            high = scaled.astype(jnp.bfloat16)
            low = (scaled - high.astype(jnp.float32)).astype(jnp.bfloat16)
            q2 = jnp.concatenate([high, low], axis=0)
            work = [(b, u) for b in range(0, wide, block) for u in range(0, keys, tile)]

            def score(item):
                b, u = item
                return jnp.dot(
                    k_ref[u : u + tile, :], q2[:, b : b + block], preferred_element_type=jnp.float32
                )

            waiting = [score(item) for item in work[:ahead]]
            done = []
            for n, (b, u) in enumerate(work):
                if n + ahead < len(work):
                    waiting.append(score(work[n + ahead]))
                if u == 0 and more:
                    acc = acc_in[0, :, b : b + block]
                elif u == 0:
                    acc = jnp.zeros((V_ROWS, block), jnp.float32)
                weights = jnp.exp2(waiting.pop(0)).astype(jnp.bfloat16)
                acc = acc + jnp.dot(
                    v_ref[:, u : u + tile], weights, preferred_element_type=jnp.float32
                )
                if u + tile == keys:
                    done.append(acc)
            finish(jnp.concatenate(done, axis=1), jnp.zeros((8, wide), jnp.float32))

        @pl.when(jnp.logical_not(limit <= 60.0))
        def _():
            step_rows = 512

            def step(u, carry):
                top, acc = carry
                rows = pl.ds(pl.multiple_of(u * step_rows, step_rows), step_rows)
                scores = (
                    jnp.dot(k_ref[rows, :HEAD], q, preferred_element_type=jnp.float32) * 0.125
                )
                new_top = jnp.maximum(top, jnp.max(scores, axis=0, keepdims=True))
                weights = jnp.exp(scores - new_top).astype(jnp.bfloat16)
                part = jnp.dot(v_ref[:, rows], weights, preferred_element_type=jnp.float32)
                return new_top, acc * jnp.exp(top - new_top) + part

            if more:
                start = (top_in[0, 0:1, :], acc_in[0])
            else:
                start = (
                    jnp.full((1, wide), -1e30, jnp.float32),
                    jnp.zeros((V_ROWS, wide), jnp.float32),
                )
            top, acc = lax.fori_loop(0, keys // step_rows, step, start)
            finish(acc, jnp.broadcast_to(top, (8, wide)))

    def whole(array, at):
        return pl.BlockSpec((array.shape[0], 2 * HEAD, TOK), lambda n, place: (0, at, 0))

    sums = [
        pl.BlockSpec((1, V_ROWS, wide), lambda n, place: (place[n], 0, 0)),
        pl.BlockSpec((1, 8, wide), lambda n, place: (place[n], 0, 0)),
    ]
    gain = pl.BlockSpec((1, HEAD), lambda n, place: (0, 0))
    result = pl.BlockSpec((GROUP * HEAD, TOK), lambda n, place: (0, 0))
    return pl.pallas_call(
        kern,
        grid_spec=pltpu.PrefetchScalarGridSpec(
            num_scalar_prefetch=1,
            grid=(places,),
            in_specs=[
                gain,
                gain,
                pl.BlockSpec((1, GROUP * HEAD, TOK), lambda n, place: (place[n], 0, 0)),
                *[whole(p, 0 if p.shape[1] == 2 * HEAD else 2) for p in pieces],
                *(sums if more else []),
            ],
            out_specs=[result] * places if last else sums,
            scratch_shapes=[
                pltpu.VMEM((keys, 2 * HEAD), jnp.bfloat16),
                pltpu.VMEM((V_ROWS, keys), jnp.bfloat16),
            ],
        ),
        out_shape=[jax.ShapeDtypeStruct((GROUP * HEAD, TOK), jnp.bfloat16)] * places
        if last
        else [
            jax.ShapeDtypeStruct((4, V_ROWS, wide), jnp.float32),
            jax.ShapeDtypeStruct((4, 8, wide), jnp.float32),
        ],
        compiler_params=pltpu.CompilerParams(vmem_limit_bytes=ATTEND_VMEM),
        cost_estimate=pl.CostEstimate(
            flops=4 * places * keys * wide * 256 * 2,
            bytes_accessed=2 * keys * 2 * HEAD,
            transcendentals=places * keys * wide,
        ),
    )(place, q_gain, k_gain, qkv, *pieces, *(before or []))


def mix(where, attended, mine, theirs):
    count = len(mine)

    def kern(where_ref, *refs):
        heads = refs[:4]
        refs = refs[4:]
        out_ref, full_ref, att_ref = refs[2 * count :]
        place = [where_ref[i] for i in range(4)]
        lay_out(place, refs[:count], refs[count : 2 * count], full_ref, pair_order)
        groups = ring_order(jnp.where(place[3] == 0, place[1], place[0]))
        for group, source in zip(groups, heads):
            at = pl.multiple_of(group * GROUP * HEAD, GROUP * HEAD)
            att_ref[pl.ds(at, GROUP * HEAD), :] = source[...]
        rows = att_ref[...].T
        out_ref[...] = lax.dot_general(
            rows, full_ref[...], (((1,), (1,)), ((), ())), preferred_element_type=jnp.float32
        ).astype(jnp.bfloat16)

    def piece(array):
        return pl.BlockSpec(array.shape, lambda: (0, 0))

    return pl.pallas_call(
        kern,
        in_specs=[
            pl.BlockSpec(memory_space=pltpu.SMEM),
            *[piece(a) for a in attended],
            *[piece(a) for a in mine],
            *[piece(a) for a in theirs],
        ],
        out_specs=pl.BlockSpec((TOK, MODEL), lambda: (0, 0)),
        out_shape=jax.ShapeDtypeStruct((TOK, MODEL), jnp.bfloat16),
        scratch_shapes=[
            pltpu.VMEM((MODEL, OUT_IN), jnp.bfloat16),
            pltpu.VMEM((OUT_IN, TOK), jnp.bfloat16),
        ],
        compiler_params=pltpu.CompilerParams(vmem_limit_bytes=24 * 2**20),
        cost_estimate=pl.CostEstimate(
            flops=2 * TOK * MODEL * OUT_IN, bytes_accessed=2 * MODEL * OUT_IN, transcendentals=0
        ),
        name="mix",
    )(where, *attended, *mine, *theirs)


def rotation_tables(offset):
    quarter = HEAD // 4
    positions = jnp.arange(TOK, dtype=jnp.int32) + offset
    frequency = rope_base ** (-jnp.arange(quarter, dtype=jnp.float32) / quarter)
    parts = []
    for coords in (positions // GRID_W, positions % GRID_W):
        angles = coords.astype(jnp.float32)[None, :] * frequency[:, None]
        parts += [jnp.cos(angles), jnp.sin(angles)]
    return jnp.concatenate(parts, axis=0)


def per_device(tokens, q_weight, k_weight, v_weight, out_weight, q_gain, k_gain):
    sp = lax.axis_index("sp")
    dp = lax.axis_index("dp")
    where = jnp.stack([sp // 4, sp % 4, dp // 2, dp % 2]).astype(jnp.int32)
    tables = rotation_tables(sp * TOK)
    q_row = q_gain.reshape(1, HEAD)
    k_row = k_gain.reshape(1, HEAD)

    own = jnp.concatenate([q_weight, k_weight, v_weight, out_weight.T], axis=1)
    block = jnp.concatenate([own, *[shift(own, ("y", "y"), -s) for s in SHIFTS[1:]]], axis=0)
    left = shift(block, INNER, 1)
    right = shift(block, INNER, -1)
    middle = block.shape[0] // 2
    far_top = shift(left[:middle], INNER, 1)
    far_bottom = shift(right[middle:], INNER, -1)
    half = jnp.concatenate([block, left], axis=0)
    other = jnp.concatenate([right, far_top, far_bottom], axis=0)
    tables, where, half, other = lax.optimization_barrier((tables, where, half, other))

    in_mine = [half[:, :QKV], other[:, :QKV]]
    in_mine += ring(*in_mine, OUTER)
    in_theirs = [swap(a) for a in in_mine]
    qkv = project(where, tokens[0], in_mine, in_theirs, tables, q_row, k_row)

    out_own = jnp.concatenate([half[:, QKV:], other[:, QKV:]], axis=0)
    qkv, out_own = lax.optimization_barrier(
        (
            lax.all_to_all(
                qkv, AXES, split_axis=0, concat_axis=0, tiled=True, axis_index_groups=EXCHANGE
            ),
            out_own,
        )
    )
    every = jnp.arange(4, dtype=jnp.int32)
    here = jnp.where(dp % 2 == 0, sp % 4, sp // 4).astype(jnp.int32)
    away = jnp.stack(ring_order(here)[1:])
    kv_own = qkv[:, GROUP * HEAD :, :]
    kv_near = pair(kv_own, OUTER, False)
    kv_next = pair(kv_own, OUTER, True)
    out_near = pair(out_own, OUTER, False)
    sums = attend(every, q_row, k_row, qkv, [qkv], None, False)
    sums, kv_near, kv_next = lax.optimization_barrier((sums, kv_near, kv_next))
    kv_far = pair(kv_near, OUTER, True)
    sums = attend(every, q_row, k_row, qkv, [kv_near], sums, False)
    sums, kv_next, kv_far, out_near = lax.optimization_barrier((sums, kv_next, kv_far, out_near))
    out_half = jnp.concatenate([out_own, out_near], axis=0)
    out_other = pair(out_half, OUTER, True)
    out_half_theirs = swap(out_half)
    behind, ahead, across = attend(away, q_row, k_row, qkv, [kv_next, kv_far], sums, True)
    sums, kv_next, kv_far, behind, ahead, across, out_half_theirs = lax.optimization_barrier(
        (sums, kv_next, kv_far, behind, ahead, across, out_half_theirs)
    )
    across = shift(across, INNER, 2)
    ahead = shift(ahead, INNER, 1)
    behind = shift(behind, INNER, -1)
    (own,) = attend(here.reshape(1), q_row, k_row, qkv, [kv_next, kv_far], sums, True)
    own, out_other = lax.optimization_barrier((own, out_other))
    out_other_theirs = swap(out_other)
    return mix(
        where, [own, ahead, behind, across], [out_half, out_other], [out_half_theirs, out_other_theirs]
    )[None]


def solution(mesh):
    return jax.shard_map(
        per_device,
        mesh=mesh,
        in_specs=(
            P("dp", "sp", None),
            P(("sp", "dp"), None),
            P(("sp", "dp"), None),
            P(("sp", "dp"), None),
            P(None, ("sp", "dp")),
            P(),
            P(),
        ),
        out_specs=P("dp", "sp", None),
        check_vma=False,
    )
```

```python
import jax
import jax.numpy as jnp
import numpy as np
from jax import lax
from jax.experimental import pallas as pl
from jax.experimental.pallas import tpu as pltpu
from jax.sharding import PartitionSpec as P

GRID_W = 64
LOG2E = 1.4426950408889634
V_ROWS = 80
ATTEND_VMEM = 24 * 2**20
HEAD = 64
KV_HEADS = 4
GROUP = 4
TOK = 384
WIDE = 384
QKV = KV_HEADS * WIDE
OUT_IN = 1024
MODEL = 2048

epsilon = 1e-06
rope_base = 10000.0

AXES = ("sp", "dp")
DEVICE = np.arange(128).reshape(4, 4, 4, 2)
SHIFTS = (0, -1, 1, 2)


def lines(axis, core):
    return np.moveaxis(DEVICE[..., core], "zxy".index(axis), -1).reshape(-1, 4).tolist()


def shift_pairs(axis_of_core, step):
    pairs = []
    for core, axis in enumerate(axis_of_core):
        for line in lines(axis, core):
            pairs += [(line[i], line[(i + step) % 4]) for i in range(4)]
    return pairs


INNER = ("x", "z")
OUTER = ("z", "x")
SWAP = [(int(i), int(i) ^ 1) for i in range(128)]
EXCHANGE = lines("x", 0) + lines("z", 1)


def shift(array, axis_of_core, step):
    return lax.ppermute(array, AXES, shift_pairs(axis_of_core, step))


def pair(array, axis_of_core, far):
    pairs = []
    for core, axis in enumerate(axis_of_core):
        for line in lines(axis, core):
            pairs += [(line[i], line[3 - i if far else i ^ 1]) for i in range(4)]
    return lax.ppermute(array, AXES, pairs)


def swap(array):
    return lax.ppermute(array, AXES, SWAP)


def ring(top, bottom, axis_of_core):
    left_top = shift(top, axis_of_core, 1)
    right_bottom = shift(bottom, axis_of_core, -1)
    left_bottom = shift(bottom, axis_of_core, 1)
    right_top = shift(top, axis_of_core, -1)
    far_top = shift(left_top, axis_of_core, 1)
    far_bottom = shift(right_bottom, axis_of_core, -1)
    return left_top, left_bottom, right_top, right_bottom, far_top, far_bottom


def ring_order(at):
    return [(at + s + 4) % 4 for s in SHIFTS]


def pair_order(at):
    near = at + 1 - 2 * (at % 2)
    return [at, near, 3 - at, 3 - near]


def lay_out(where, mine, theirs, full_ref, outer_order):
    z, x, y, own_core = where
    y_at = ring_order(y)
    for pieces, core in ((mine, own_core), (theirs, 1 - own_core)):
        first = core == 0
        outer_at = outer_order(jnp.where(first, z, x))
        inner_at = ring_order(jnp.where(first, x, z))
        stack = [(p, r) for p in pieces for r in range(0, p.shape[0], 16)]
        for outer in range(4):
            for inner in range(4):
                z_at = jnp.where(first, outer_at[outer], inner_at[inner])
                x_at = jnp.where(first, inner_at[inner], outer_at[outer])
                base = (z_at * 4 + x_at) * 128 + core * 16
                for step in range(4):
                    source, row = stack[outer * 16 + inner * 4 + step]
                    at = pl.multiple_of(base + y_at[step] * 32, 16)
                    full_ref[pl.ds(at, 16), :] = source[row : row + 16, :]


def column(row):
    size = row.shape[1]
    diagonal = lax.broadcasted_iota(jnp.int32, (size, size), 0) == lax.broadcasted_iota(
        jnp.int32, (size, size), 1
    )
    return jnp.sum(jnp.where(diagonal, row, 0.0), axis=1, keepdims=True)


def project(where, tokens, mine, theirs, tables, q_gain, k_gain):
    count = len(mine)

    def kern(where_ref, tok_ref, *refs):
        table_ref, qg_ref, kg_ref, out_ref, full_ref = refs[2 * count :]
        place = [where_ref[i] for i in range(4)]
        lay_out(place, refs[:count], refs[count : 2 * count], full_ref, ring_order)
        cos_r, sin_r = table_ref[0:16, :], table_ref[16:32, :]
        cos_c, sin_c = table_ref[32:48, :], table_ref[48:64, :]
        gains = (column(qg_ref[...]), column(kg_ref[...]))
        tok = tok_ref[...]
        heads = GROUP * KV_HEADS
        for pair in range((heads + 2 * KV_HEADS) // 2):
            cols = slice(pair * 2 * HEAD, (pair + 1) * 2 * HEAD)
            if pair % 2 == 0:
                both = slice(cols.start, cols.start + 4 * HEAD)
                raw = jnp.dot(tok, full_ref[:, both], preferred_element_type=jnp.float32)
            flat = raw[:, (pair % 2) * 2 * HEAD : (pair % 2 + 1) * 2 * HEAD].T
            for i in range(2):
                head = 2 * pair + i
                v = flat[i * HEAD : (i + 1) * HEAD, :]
                if head < heads + KV_HEADS:
                    mean_sq = jnp.mean(v * v, axis=0, keepdims=True)
                    v = v * lax.rsqrt(mean_sq + epsilon) * gains[head // heads]
                    a, b, c, d = v[0:16], v[16:32], v[32:48], v[48:64]
                    v = jnp.concatenate(
                        [
                            a * cos_r - b * sin_r,
                            b * cos_r + a * sin_r,
                            c * cos_c - d * sin_c,
                            d * cos_c + c * sin_c,
                        ],
                        axis=0,
                    )
                if head < heads:
                    group, at = head // GROUP, head % GROUP
                else:
                    group, at = head % KV_HEADS, GROUP + (head - heads) // KV_HEADS
                out_ref[group, at * HEAD : (at + 1) * HEAD, :] = v.astype(jnp.bfloat16)

    return pl.pallas_call(
        kern,
        in_specs=[pl.BlockSpec(memory_space=pltpu.SMEM)]
        + [pl.BlockSpec(memory_space=pltpu.VMEM)] * (2 * count + 4),
        out_specs=pl.BlockSpec(memory_space=pltpu.VMEM),
        out_shape=jax.ShapeDtypeStruct((KV_HEADS, WIDE, TOK), jnp.bfloat16),
        scratch_shapes=[pltpu.VMEM((MODEL, QKV), jnp.bfloat16)],
        compiler_params=pltpu.CompilerParams(vmem_limit_bytes=28 * 2**20),
        cost_estimate=pl.CostEstimate(
            flops=2 * TOK * MODEL * QKV, bytes_accessed=2 * MODEL * QKV, transcendentals=0
        ),
        name="project",
    )(where, tokens, *mine, *theirs, tables, q_gain, k_gain)


def attend(place, q_gain, k_gain, qkv, pieces, before, last):
    keys = sum(p.shape[0] for p in pieces) * TOK
    places = place.shape[0]
    tile = 256
    block = 512
    ahead = 2
    wide = GROUP * TOK
    more = before is not None

    def kern(place_ref, qg_ref, kg_ref, q_ref, *refs):
        sources = refs[: len(pieces)]
        rest = refs[len(pieces) :]
        if more:
            acc_in, top_in = rest[:2]
            rest = rest[2:]
        *outs, k_ref, v_ref = rest

        @pl.when(pl.program_id(0) == 0)
        def _():
            at = 0
            for source in sources:
                for i in range(source.shape[0]):
                    k = source[i, 0:HEAD, :]
                    k_ref[at : at + TOK, :] = jnp.concatenate([k, k], axis=0).T
                    v_ref[0:HEAD, at : at + TOK] = source[i, HEAD : 2 * HEAD, :]
                    at += TOK
            row = lax.broadcasted_iota(jnp.int32, (V_ROWS - HEAD, keys), 0)
            v_ref[HEAD:, :] = jnp.where(row == 0, 1.0, 0.0).astype(jnp.bfloat16)

        q = jnp.concatenate([q_ref[0, h * HEAD : (h + 1) * HEAD, :] for h in range(GROUP)], axis=1)
        limit = 8.0 * jnp.max(jnp.abs(qg_ref[...])) * jnp.max(jnp.abs(kg_ref[...]))

        def finish(acc, top):
            if not last:
                outs[0][0] = acc
                outs[1][0] = top
                return
            result = (acc[:HEAD] / acc[HEAD : HEAD + 1]).astype(jnp.bfloat16)
            for n in range(places):

                @pl.when(pl.program_id(0) == n)
                def _():
                    for h in range(GROUP):
                        outs[n][h * HEAD : (h + 1) * HEAD, :] = result[:, h * TOK : (h + 1) * TOK]

        @pl.when(limit <= 60.0)
        def _():
            scaled = q.astype(jnp.float32) * (0.125 * LOG2E)
            high = scaled.astype(jnp.bfloat16)
            low = (scaled - high.astype(jnp.float32)).astype(jnp.bfloat16)
            q2 = jnp.concatenate([high, low], axis=0)
            work = [(b, u) for b in range(0, wide, block) for u in range(0, keys, tile)]

            def score(item):
                b, u = item
                return jnp.dot(
                    k_ref[u : u + tile, :], q2[:, b : b + block], preferred_element_type=jnp.float32
                )

            waiting = [score(item) for item in work[:ahead]]
            done = []
            for n, (b, u) in enumerate(work):
                if n + ahead < len(work):
                    waiting.append(score(work[n + ahead]))
                if u == 0 and more:
                    acc = acc_in[0, :, b : b + block]
                elif u == 0:
                    acc = jnp.zeros((V_ROWS, block), jnp.float32)
                weights = jnp.exp2(waiting.pop(0)).astype(jnp.bfloat16)
                acc = acc + jnp.dot(
                    v_ref[:, u : u + tile], weights, preferred_element_type=jnp.float32
                )
                if u + tile == keys:
                    done.append(acc)
            finish(jnp.concatenate(done, axis=1), jnp.zeros((8, wide), jnp.float32))

        @pl.when(jnp.logical_not(limit <= 60.0))
        def _():
            step_rows = 512

            def step(u, carry):
                top, acc = carry
                rows = pl.ds(pl.multiple_of(u * step_rows, step_rows), step_rows)
                scores = (
                    jnp.dot(k_ref[rows, :HEAD], q, preferred_element_type=jnp.float32) * 0.125
                )
                new_top = jnp.maximum(top, jnp.max(scores, axis=0, keepdims=True))
                weights = jnp.exp(scores - new_top).astype(jnp.bfloat16)
                part = jnp.dot(v_ref[:, rows], weights, preferred_element_type=jnp.float32)
                return new_top, acc * jnp.exp(top - new_top) + part

            if more:
                start = (top_in[0, 0:1, :], acc_in[0])
            else:
                start = (
                    jnp.full((1, wide), -1e30, jnp.float32),
                    jnp.zeros((V_ROWS, wide), jnp.float32),
                )
            top, acc = lax.fori_loop(0, keys // step_rows, step, start)
            finish(acc, jnp.broadcast_to(top, (8, wide)))

    def whole(array, at):
        return pl.BlockSpec((array.shape[0], 2 * HEAD, TOK), lambda n, place: (0, at, 0))

    sums = [
        pl.BlockSpec((1, V_ROWS, wide), lambda n, place: (place[n], 0, 0)),
        pl.BlockSpec((1, 8, wide), lambda n, place: (place[n], 0, 0)),
    ]
    gain = pl.BlockSpec((1, HEAD), lambda n, place: (0, 0))
    result = pl.BlockSpec((GROUP * HEAD, TOK), lambda n, place: (0, 0))
    return pl.pallas_call(
        kern,
        grid_spec=pltpu.PrefetchScalarGridSpec(
            num_scalar_prefetch=1,
            grid=(places,),
            in_specs=[
                gain,
                gain,
                pl.BlockSpec((1, GROUP * HEAD, TOK), lambda n, place: (place[n], 0, 0)),
                *[whole(p, 0 if p.shape[1] == 2 * HEAD else 2) for p in pieces],
                *(sums if more else []),
            ],
            out_specs=[result] * places if last else sums,
            scratch_shapes=[
                pltpu.VMEM((keys, 2 * HEAD), jnp.bfloat16),
                pltpu.VMEM((V_ROWS, keys), jnp.bfloat16),
            ],
        ),
        out_shape=[jax.ShapeDtypeStruct((GROUP * HEAD, TOK), jnp.bfloat16)] * places
        if last
        else [
            jax.ShapeDtypeStruct((4, V_ROWS, wide), jnp.float32),
            jax.ShapeDtypeStruct((4, 8, wide), jnp.float32),
        ],
        compiler_params=pltpu.CompilerParams(vmem_limit_bytes=ATTEND_VMEM),
        cost_estimate=pl.CostEstimate(
            flops=4 * places * keys * wide * 256 * 2,
            bytes_accessed=2 * keys * 2 * HEAD,
            transcendentals=places * keys * wide,
        ),
    )(place, q_gain, k_gain, qkv, *pieces, *(before or []))


def mix(where, attended, mine, theirs):
    count = len(mine)

    def kern(where_ref, *refs):
        heads = refs[:4]
        refs = refs[4:]
        out_ref, full_ref, att_ref = refs[2 * count :]
        place = [where_ref[i] for i in range(4)]
        lay_out(place, refs[:count], refs[count : 2 * count], full_ref, pair_order)
        groups = ring_order(jnp.where(place[3] == 0, place[1], place[0]))
        for group, source in zip(groups, heads):
            at = pl.multiple_of(group * GROUP * HEAD, GROUP * HEAD)
            att_ref[pl.ds(at, GROUP * HEAD), :] = source[...]
        rows = att_ref[...].T
        out_ref[...] = lax.dot_general(
            rows, full_ref[...], (((1,), (1,)), ((), ())), preferred_element_type=jnp.float32
        ).astype(jnp.bfloat16)

    def piece(array):
        return pl.BlockSpec(array.shape, lambda: (0, 0))

    return pl.pallas_call(
        kern,
        in_specs=[
            pl.BlockSpec(memory_space=pltpu.SMEM),
            *[piece(a) for a in attended],
            *[piece(a) for a in mine],
            *[piece(a) for a in theirs],
        ],
        out_specs=pl.BlockSpec((TOK, MODEL), lambda: (0, 0)),
        out_shape=jax.ShapeDtypeStruct((TOK, MODEL), jnp.bfloat16),
        scratch_shapes=[
            pltpu.VMEM((MODEL, OUT_IN), jnp.bfloat16),
            pltpu.VMEM((OUT_IN, TOK), jnp.bfloat16),
        ],
        compiler_params=pltpu.CompilerParams(vmem_limit_bytes=24 * 2**20),
        cost_estimate=pl.CostEstimate(
            flops=2 * TOK * MODEL * OUT_IN, bytes_accessed=2 * MODEL * OUT_IN, transcendentals=0
        ),
        name="mix",
    )(where, *attended, *mine, *theirs)


def rotation_tables(offset):
    quarter = HEAD // 4
    positions = jnp.arange(TOK, dtype=jnp.int32) + offset
    frequency = rope_base ** (-jnp.arange(quarter, dtype=jnp.float32) / quarter)
    parts = []
    for coords in (positions // GRID_W, positions % GRID_W):
        angles = coords.astype(jnp.float32)[None, :] * frequency[:, None]
        parts += [jnp.cos(angles), jnp.sin(angles)]
    return jnp.concatenate(parts, axis=0)


def per_device(tokens, q_weight, k_weight, v_weight, out_weight, q_gain, k_gain):
    sp = lax.axis_index("sp")
    dp = lax.axis_index("dp")
    where = jnp.stack([sp // 4, sp % 4, dp // 2, dp % 2]).astype(jnp.int32)
    tables = rotation_tables(sp * TOK)
    q_row = q_gain.reshape(1, HEAD)
    k_row = k_gain.reshape(1, HEAD)

    own = jnp.concatenate([q_weight, k_weight, v_weight, out_weight.T], axis=1)
    block = jnp.concatenate([own, *[shift(own, ("y", "y"), -s) for s in SHIFTS[1:]]], axis=0)
    left = shift(block, INNER, 1)
    right = shift(block, INNER, -1)
    middle = block.shape[0] // 2
    far_top = shift(left[:middle], INNER, 1)
    far_bottom = shift(right[middle:], INNER, -1)
    half = jnp.concatenate([block, left], axis=0)
    other = jnp.concatenate([right, far_top, far_bottom], axis=0)
    tables, where, half, other = lax.optimization_barrier((tables, where, half, other))

    in_mine = [half[:, :QKV], other[:, :QKV]]
    in_mine += ring(*in_mine, OUTER)
    in_theirs = [swap(a) for a in in_mine]
    qkv = project(where, tokens[0], in_mine, in_theirs, tables, q_row, k_row)

    out_own = jnp.concatenate([half[:, QKV:], other[:, QKV:]], axis=0)
    qkv, out_own = lax.optimization_barrier(
        (
            lax.all_to_all(
                qkv, AXES, split_axis=0, concat_axis=0, tiled=True, axis_index_groups=EXCHANGE
            ),
            out_own,
        )
    )
    every = jnp.arange(4, dtype=jnp.int32)
    here = jnp.where(dp % 2 == 0, sp % 4, sp // 4).astype(jnp.int32)
    away = jnp.stack(ring_order(here)[1:])
    kv_own = qkv[:, GROUP * HEAD :, :]
    kv_near = pair(kv_own, OUTER, False)
    kv_next = pair(kv_own, OUTER, True)
    out_near = pair(out_own, OUTER, False)
    sums = attend(every, q_row, k_row, qkv, [qkv], None, False)
    sums, kv_near, kv_next = lax.optimization_barrier((sums, kv_near, kv_next))
    kv_far = pair(kv_near, OUTER, True)
    first_sums = sums
    sums = attend(away, q_row, k_row, qkv, [kv_near], sums, False)
    sums, kv_next, kv_far, out_near = lax.optimization_barrier((sums, kv_next, kv_far, out_near))
    out_half = jnp.concatenate([out_own, out_near], axis=0)
    out_other = pair(out_half, OUTER, True)
    out_half_theirs = swap(out_half)
    behind, ahead, across = attend(away, q_row, k_row, qkv, [kv_next, kv_far], sums, True)
    first_sums, kv_next, kv_far, behind, ahead, across, out_half_theirs = lax.optimization_barrier(
        (first_sums, kv_next, kv_far, behind, ahead, across, out_half_theirs)
    )
    across = shift(across, INNER, 2)
    ahead = shift(ahead, INNER, 1)
    behind = shift(behind, INNER, -1)
    (own,) = attend(here.reshape(1), q_row, k_row, qkv, [kv_near, kv_next, kv_far], first_sums, True)
    own, out_other = lax.optimization_barrier((own, out_other))
    out_other_theirs = swap(out_other)
    return mix(
        where, [own, ahead, behind, across], [out_half, out_other], [out_half_theirs, out_other_theirs]
    )[None]


def solution(mesh):
    return jax.shard_map(
        per_device,
        mesh=mesh,
        in_specs=(
            P("dp", "sp", None),
            P(("sp", "dp"), None),
            P(("sp", "dp"), None),
            P(("sp", "dp"), None),
            P(None, ("sp", "dp")),
            P(),
            P(),
        ),
        out_specs=P("dp", "sp", None),
        check_vma=False,
    )
```
